32 devices in a mesh: ep: 8 (over z, y), tp: 4 (over x, core).
Axes of the slice: x: 2, y: 2, z: 4, core: 2. Of those that a mesh axis runs over, the one named last changes fastest.
Arguments:
- conv_value: bfloat16 [4096, 2048], P('ep', 'tp'), may hold values from -6 to 6
- conv_gate: bfloat16 [4096, 2048], P('ep', 'tp'), may hold values from -9 to 9
- conv_kernel: float32 [31, 2048], P(None, 'tp'), may hold values from -20 to 20
- norm_gain: float32 [2048], P('tp'), may hold values from 0.1 to 1.9
- mixer_proj: bfloat16 [2048, 2048], P('tp'), may hold values from -0.125 to 0.125
- moe_in: bfloat16 [4096, 2048], P('ep'), may hold values from -6 to 6
- route_ids: int32 [4096, 2], P('ep'), may hold values from 0 to 7, all different within a row; in each aligned block of 128 rows (0 to 127, 128 to 255, ...) at most 64 rows name the same one
- route_logits: float32 [4096, 2], P('ep'), may hold values from -6 to 6
- moe_gain: float32 [2048], replicated, may hold values from 0.1 to 1.9
- expert_gate: bfloat16 [8, 2048, 2048], P('ep', None, 'tp'), may hold values from -0.26367188 to 0.26367188
- expert_lin: bfloat16 [8, 2048, 2048], P('ep', None, 'tp'), may hold values from -0.26367188 to 0.26367188
- expert_down: bfloat16 [8, 2048, 2048], P('ep', 'tp'), may hold values from -0.052978516 to 0.052978516
Outputs:
- mixer_out: bfloat16 [4096, 2048], P(('ep', 'tp'))
- moe_out: bfloat16 [4096, 2048], P(('ep', 'tp'))
The draws below stay inside these ranges and needn't reach their ends.
Inputs may be any that keep to these rules, and one draw needn't show every extreme that they name: `route_ids`: every row names 2 different experts. In each aligned block of 128 rows (one device's output rows) no expert is named by more than 64 rows, and in every draw some expert is named by exactly 64 rows of some block.
All inputs are finite; a program needn't handle non-finite values.
Results may differ from the reference program's by a relative error of at most 0.01.
Values may be sent and summed in bfloat16 or wider, within the bound.
A program may use at most 128 MiB of HBM per device.

```python
import math
import jax
import jax.numpy as jnp
import numpy as np
from jax import lax

D = 2048
C = 2048
F = 2048
KW = 31
TOPK = 2
ROWS = 128
EXPERTS = 8
CAP = 64
TOKM = 4096
TOKE = 4096
N_TP = 4


def draw_conv_kernel(key, part):
    first = jax.random.fold_in(key, 11)
    second = jax.random.fold_in(key, 12)
    base = jax.random.normal(first, (KW, C), jnp.float32)
    spread = jnp.exp(jax.random.uniform(second, (1, C), jnp.float32, -0.5, 0.5))
    rising = jnp.exp(math.log(10.0) * jnp.arange(C, dtype=jnp.float32) / C)[None, :]
    return base * spread * rising / math.sqrt(KW)


def levels(key, shape, pieces, low, top_value):
    factor_of, own = 1.0, jax.random.fold_in(key, 6)
    for position, shards_of in pieces:
        steps = jnp.exp(jax.random.uniform(jax.random.fold_in(own, position), (shards_of,), jnp.float32, low / len(pieces), top_value / len(pieces)))
        factor_of = factor_of * jnp.repeat(steps, shape[position] // shards_of).reshape([-1 if axis == position else 1 for axis in range(len(shape))])
    return factor_of


def routed_block(own_key, own, number, rows, count, top, bound, slope):
    order = jax.random.permutation(own_key, count)
    heavy_load, common = portions_of(count, rows * top, bound, slope, True), portions_of(count, rows * top, bound, slope, False)
    places = jnp.arange(count)

    def named(lengths, turn):
        used = int((lengths > 0).sum())
        fixed = max(1, used // 4)
        moved = fixed + (places - fixed + turn * (used - fixed)) % max(1, count - fixed)
        return jnp.zeros((count,), jnp.int32).at[order[jnp.where(places < fixed, places, moved)]].set(jnp.asarray(lengths, jnp.int32))

    lengths = jnp.where(number % 4 == 0, named(heavy_load, number // 4), named(common, number - number // 4 - 1))
    mixed = jax.random.permutation(jax.random.fold_in(own, 3), count)
    giver, sink = mixed[0:count // 2 * 2:2], mixed[1:count // 2 * 2:2]
    slack = jnp.minimum(lengths[giver] - 1, bound - lengths[sink]) // 2
    slack = jnp.where((giver == order[0]) | (sink == order[0]) | (lengths[sink] == 0), 0, jnp.maximum(slack, 0))
    moved = jax.random.randint(jax.random.fold_in(own, 4), (count // 2,), 0, 1 << 20) % (slack + 1)
    lengths = lengths.at[giver].add(-moved).at[sink].add(moved)
    items = jnp.searchsorted(jnp.cumsum(lengths), jnp.arange(rows * top), side="right").astype(jnp.int32)
    table = items.reshape(top, rows).T
    table = table[jax.random.permutation(jax.random.fold_in(own, 1), rows)]
    turn = jax.random.randint(jax.random.fold_in(own, 2), (rows, 1), 0, top)
    return jnp.take_along_axis(table, (jnp.arange(top)[None, :] + turn) % top, axis=1)


def portions_of(number_of, total, reach, skew, full):
    portions = [(1 << 20) // math.isqrt(standing ** skew) + 1 for standing in range(1, number_of + 1)]
    largest = reach if full else min(reach, max(-(-total // number_of), total * portions[0] // sum(portions)))
    least = 1 if total - largest >= number_of - 1 else 0
    given, surplus = [largest] + [least] * (number_of - 1), total - largest - least * (number_of - 1)
    while surplus > 0:
        candidates = [i for i in range(1, number_of) if given[i] < largest] or [i for i in range(1, number_of) if given[i] < reach]
        whole, remaining = sum([portions[i] for i in candidates]), surplus
        for i in candidates:
            more = min(reach - given[i], max(1, remaining * portions[i] // whole), surplus)
            given[i] = given[i] + more
            surplus = surplus - more
    return np.array(given)


def gaussian(rng, shape, width, limit, shards=(), kind=jnp.bfloat16):
    result = jax.random.normal(rng, shape, jnp.float32) * width
    if len(shards) > 0:
        result = levels(rng, shape, shards, -0.22, 0.18) * result
    return jnp.clip(result, min=-limit, max=limit).astype(kind)


def setup_inputs(seed: int = 0) -> dict:
    keys = jax.random.split(jax.random.key(seed), 13)
    conv_value = gaussian(keys[0], (TOKM, C), 1.0, 6.0, ((0, 8), (1, 4)))
    conv_gate = gaussian(keys[1], (TOKM, C), 1.5, 9.0, ((0, 8), (1, 4)))
    conv_kernel = draw_conv_kernel(jax.random.fold_in(keys[12], 71), 0)
    norm_gain = jnp.clip(1.0 + 0.18 * jax.random.normal(keys[3], (C,), jnp.float32), 0.1, 1.9)
    mixer_proj = gaussian(keys[4], (C, D), C ** -0.5, 0.125, ((0, 4),))
    moe_in = gaussian(keys[5], (TOKE, D), 1.0, 6.0, ((0, 8),))
    route_ids_keys = jax.random.split(jax.random.fold_in(keys[6], 1), TOKE // ROWS)
    route_ids_turns = jax.random.permutation(jax.random.fold_in(keys[6], 3), TOKE // ROWS)
    route_ids = jax.vmap(lambda own, number: routed_block(jax.random.fold_in(keys[6], 2), own, number, ROWS, EXPERTS, TOPK, CAP, 1))(route_ids_keys, route_ids_turns).reshape((TOKE, TOPK))
    route_logits = gaussian(keys[7], (TOKE, TOPK), 1.5, 6.0, ((0, 8),), jnp.float32)
    moe_gain = jnp.clip(1.0 + 0.18 * jax.random.normal(keys[8], (D,), jnp.float32), 0.1, 1.9)
    expert_gate = gaussian(keys[9], (EXPERTS, D, F), (2.0 * D ** -0.5), 0.26367188, ((0, 8), (2, 4)))
    expert_lin = gaussian(keys[10], (EXPERTS, D, F), (2.0 * D ** -0.5), 0.26367188, ((0, 8), (2, 4)))
    expert_down = gaussian(keys[11], (EXPERTS, F, D), (0.4 * F ** -0.5), 0.052978516, ((0, 8), (1, 4)))
    return {"conv_value": conv_value, "conv_gate": conv_gate, "conv_kernel": conv_kernel, "norm_gain": norm_gain, "mixer_proj": mixer_proj, "moe_in": moe_in, "route_ids": route_ids, "route_logits": route_logits, "moe_gain": moe_gain, "expert_gate": expert_gate, "expert_lin": expert_lin, "expert_down": expert_down}


EPS = 1e-05
LIMIT = 7.0
SLOPE = 1.702

def slot_targets(routes, experts, capacity):
    flat = routes.reshape(-1)
    onehot = (flat[:, None] == jnp.arange(experts, dtype=jnp.int32)[None, :]).astype(jnp.int32)
    rank = lax.optimization_barrier(jnp.sum(jnp.cumsum(onehot, axis=0) * onehot, axis=1)) - 1
    return (flat * capacity + rank).astype(jnp.int32)

def slot_sources(target, total, topk):
    hits = (target[None, :] == jnp.arange(total, dtype=jnp.int32)[:, None]).astype(jnp.int32)
    owner = jnp.arange(target.shape[0], dtype=jnp.int32) // topk
    source = lax.optimization_barrier(jnp.sum(hits * owner[None, :], axis=1)).astype(jnp.int32)
    filled = lax.optimization_barrier(jnp.sum(hits, axis=1)) > 0
    return (source, filled)

def reference(conv_value, conv_gate, conv_kernel, norm_gain, mixer_proj, moe_in, route_ids, route_logits, moe_gain, expert_gate, expert_lin, expert_down):
    glu = (conv_value.astype(jnp.float32) * jax.nn.sigmoid(conv_gate.astype(jnp.float32))).astype(jnp.bfloat16)
    padded = jnp.pad(glu.astype(jnp.float32), ((KW - 1, 0), (0, 0)))
    conv = jnp.zeros((TOKM, C), jnp.float32)
    for tap in range(KW):
        conv = conv + conv_kernel[tap][None, :] * padded[tap:tap + TOKM]
    mean = lax.optimization_barrier(jnp.mean(conv, axis=1, keepdims=True))
    var = lax.optimization_barrier(jnp.mean(jnp.square(conv - mean), axis=1, keepdims=True))
    conv_act = jax.nn.silu((conv - mean) * lax.rsqrt(var + EPS) * norm_gain).astype(jnp.bfloat16)
    block_c = C // N_TP
    mixer_sum = jnp.zeros((TOKM, D), jnp.float32)
    for part in range(N_TP):
        term = jnp.dot(conv_act[:, part * block_c:(part + 1) * block_c], mixer_proj[part * block_c:(part + 1) * block_c], preferred_element_type=jnp.float32)
        mixer_sum = mixer_sum + term.astype(jnp.bfloat16).astype(jnp.float32)
    mixer_out = mixer_sum.astype(jnp.bfloat16)
    xin = moe_in.astype(jnp.float32)
    mu = lax.optimization_barrier(jnp.mean(xin, axis=1, keepdims=True))
    va = lax.optimization_barrier(jnp.mean(jnp.square(xin - mu), axis=1, keepdims=True))
    moe_norm = ((xin - mu) * lax.rsqrt(va + EPS) * moe_gain).astype(jnp.bfloat16)
    blocks = TOKE // ROWS
    routes = route_ids.reshape(blocks, ROWS, TOPK)
    targets = jax.vmap(lambda r: slot_targets(r, EXPERTS, CAP))(routes)
    sources, filled = jax.vmap(lambda t: slot_sources(t, EXPERTS * CAP, TOPK))(targets)
    base = (jnp.arange(blocks, dtype=jnp.int32) * ROWS)[:, None]
    global_src = (sources + base).reshape(blocks, EXPERTS, CAP)
    live = filled.reshape(blocks, EXPERTS, CAP)
    block_f = F // N_TP

    def one_expert(expert):
        index = lax.dynamic_index_in_dim(global_src, expert, 1, keepdims=False).reshape(-1)
        mask = lax.dynamic_index_in_dim(live, expert, 1, keepdims=False).reshape(-1)
        rows = jnp.where(mask[:, None], moe_norm[index], jnp.zeros((), jnp.bfloat16))
        gate = jnp.minimum(jnp.dot(rows, expert_gate[expert], preferred_element_type=jnp.float32), LIMIT)
        lin = jnp.clip(jnp.dot(rows, expert_lin[expert], preferred_element_type=jnp.float32), -LIMIT, LIMIT)
        hidden = (gate * jax.nn.sigmoid(SLOPE * gate) * (lin + 1.0)).astype(jnp.bfloat16)
        down = expert_down[expert]
        total = jnp.zeros((rows.shape[0], D), jnp.float32)
        for part in range(N_TP):
            term = jnp.dot(hidden[:, part * block_f:(part + 1) * block_f], down[part * block_f:(part + 1) * block_f], preferred_element_type=jnp.float32)
            total = total + term.astype(jnp.bfloat16).astype(jnp.float32)
        return total.astype(jnp.bfloat16)
    outputs = lax.map(one_expert, jnp.arange(EXPERTS, dtype=jnp.int32))
    flat_out = outputs.reshape(EXPERTS * blocks * CAP, D)
    expert_id = targets // CAP
    slot = targets % CAP
    where = (expert_id * (blocks * CAP) + jnp.arange(blocks, dtype=jnp.int32)[:, None] * CAP + slot).reshape(-1)
    picked = flat_out[where].astype(jnp.float32).reshape(TOKE, TOPK, D)
    expo = jnp.exp(route_logits)
    weight = expo / lax.optimization_barrier(jnp.sum(expo, axis=1, keepdims=True))
    moe_out = lax.optimization_barrier(jnp.sum(picked * weight[:, :, None], axis=1)).astype(jnp.bfloat16)
    return (mixer_out, moe_out)
```

```python
import jax
import jax.numpy as jnp
from jax import lax
from jax.experimental import pallas as pl
from jax.experimental.pallas import tpu as pltpu
from jax.sharding import PartitionSpec as P

EPS = 1e-05
LIMIT = 7.0
SLOPE = 1.702
F32 = jnp.float32
BF16 = jnp.bfloat16
LANES = 128
RIM = 32
NEAR = 4


def remote(src, dst, send, recv, device):
    return pltpu.make_async_remote_copy(
        src_ref=src,
        dst_ref=dst,
        send_sem=send,
        recv_sem=recv,
        device_id=device,
        device_id_type=pl.DeviceIdType.MESH,
    )


def joined(block):
    groups, rows, width = block.shape
    if rows % 16:
        return block.astype(F32).reshape(groups * rows, width).astype(BF16)
    return block.reshape(groups * rows, width)


def layer_kernel(
    ids, logits, kern, ngain, mgain,
    moe_hbm, value_hbm, cgate_hbm, gate_hbm, lin_hbm, down_hbm, proj_hbm,
    mix_out, moe_out,
    gate_w, lin_w, down_w, proj_w,
    xrows, normed, slots, weights, far_pack, near_pack,
    arrived, part, a_recv, b_send, b_recv, c_send, c_recv,
    value, cgate, padded, conv, tot, squ, act, rim_send, rim_recv, stat_send, stat_recv,
    m_part, m_a, m_bs, m_b,
    wmat, load_sem, sems, t_sems, m_sems,
):
    experts, _, cap, width = arrived.shape
    rows = moe_out.shape[0]
    length, chans = value.shape
    taps = kern.shape[0]
    groups = experts // NEAR
    ep, tp = lax.axis_index("ep"), lax.axis_index("tp")
    core, side = lax.rem(tp, 2), lax.div(tp, 2)
    xpeer, cpeer = {"tp": lax.rem(tp + 2, 4)}, {"tp": tp + 1 - 2 * core}
    dpeer = {"tp": lax.rem(tp + 3 - 2 * core, 4)}
    pos, posx = core * 2 + side, core * 2 + 1 - side
    mine = core * 2
    grp = lax.div(ep, NEAR)
    mem = lax.rem(ep, NEAR)
    row, col = lax.div(mem, 2), lax.rem(mem, 2)

    def near(k):
        return grp * NEAR + lax.rem(row + k // 2, 2) * 2 + lax.rem(col + k, 2)

    def far(j):
        other = lax.rem(grp + lax.div(j, NEAR) + 1, groups)
        k = lax.rem(j, NEAR)
        inner = jnp.where(other < grp, 1, 0)
        return other, inner, k

    def far_source(j):
        other, inner, k = far(j)
        return other * NEAR + lax.rem(inner + lax.div(k, 2), 2) * 2 + lax.rem(col + k, 2)

    def far_target(j):
        other, inner, k = far(j)
        return other * NEAR + lax.rem(inner + k, 2) * 2 + lax.rem(col + lax.div(k, 2), 2)

    def near_step(i):
        return jnp.logical_or(jnp.logical_or(i < 2, i == 3), i == experts - 1)

    def source(i):
        k = jnp.where(i < 2, i, jnp.where(i == 3, 2, 3))
        close = grp * NEAR + lax.rem(row + lax.div(k, 2), 2) * 2 + lax.rem(col + k, 2)
        distant = far_source(jnp.where(i < 4, 0, jnp.minimum(i - 3, experts - NEAR - 1)))
        return jnp.where(near_step(i), close, distant)

    loads = [
        pltpu.make_async_copy(moe_hbm.at[pl.ds(tp * rows, rows)], xrows.at[0], load_sem.at[0]),
        pltpu.make_async_copy(
            moe_hbm.at[pl.ds(lax.rem(tp + 2, 4) * rows, rows)], xrows.at[1], load_sem.at[1]
        ),
        pltpu.make_async_copy(value_hbm, value, load_sem.at[2]),
        pltpu.make_async_copy(cgate_hbm, cgate, load_sem.at[3]),
        pltpu.make_async_copy(gate_hbm, gate_w, load_sem.at[4]),
        pltpu.make_async_copy(lin_hbm, lin_w, load_sem.at[5]),
        pltpu.make_async_copy(down_hbm, down_w, load_sem.at[6]),
        pltpu.make_async_copy(proj_hbm, proj_w, load_sem.at[7]),
    ]
    for load in loads:
        load.start()

    barrier = pltpu.get_barrier_semaphore()

    @pl.loop(1, experts)
    def _(d):
        pl.semaphore_signal(
            barrier, inc=1, device_id={"ep": lax.rem(ep + d, experts)},
            device_id_type=pl.DeviceIdType.MESH,
        )

    for peer in (xpeer, cpeer, dpeer):
        pl.semaphore_signal(barrier, inc=1, device_id=peer, device_id_type=pl.DeviceIdType.MESH)

    padded_experts = -(-experts // 8) * 8
    before = (
        lax.broadcasted_iota(jnp.int32, (rows, rows), 0)
        < lax.broadcasted_iota(jnp.int32, (rows, rows), 1)
    ).astype(BF16)
    names = lax.broadcasted_iota(jnp.int32, (padded_experts, rows), 0)
    for b, block in ((0, tp), (1, lax.rem(tp + 2, 4))):
        chosen = ids[block]
        first, second = chosen[0:1] == names, chosen[1:2] == names
        taken = jnp.where(jnp.logical_or(first, second), 1.0, 0.0)
        rank = jnp.dot(taken.astype(BF16), before, preferred_element_type=F32)
        place = jnp.where(taken > 0.0, rank, -1.0)
        for e in range(experts):
            slots[b, e] = place[e : e + 1]
        if b == 0:
            expo = jnp.exp(logits[block])
            total = expo[0:1] + expo[1:2]
            share = jnp.where(first, expo[0:1] / total, 0.0) + jnp.where(
                second, expo[1:2] / total, 0.0
            )
            for e in range(experts):
                weights[e] = share[e : e + 1]

    def selected(b, group):
        order = lax.broadcasted_iota(jnp.int32, (cap, rows), 0).astype(F32)
        picks = [jnp.where(slots[b, group * NEAR + m] == order, 1.0, 0.0) for m in range(NEAR)]
        return jnp.concatenate(picks, axis=0).astype(BF16)

    for b in range(2):
        loads[b].wait()
        for r in range(0, rows, 16):
            block = xrows[b, r : r + 16].astype(F32)
            mu = jnp.mean(block, axis=1, keepdims=True)
            block = block - mu
            va = jnp.mean(jnp.square(block), axis=1, keepdims=True)
            normed[b, r : r + 16] = (block * lax.rsqrt(va + EPS) * mgain[...]).astype(BF16)

    tile = min(512, width)
    for b in range(2):
        pick = selected(b, grp)
        where = side if b == 0 else 1 - side
        for n in range(0, width, tile):
            y = jnp.dot(pick, normed[b, :, n : n + tile], preferred_element_type=F32)
            near_pack[:, where, :, n : n + tile] = y.reshape(NEAR, cap, tile).astype(BF16)

    arrived[ep, pl.ds(mine, 2)] = near_pack[mem]

    def gated(start, count, over):
        glu = value[pl.ds(start, count), over].astype(F32) * jax.nn.sigmoid(
            cgate[pl.ds(start, count), over].astype(F32)
        )
        return glu.astype(BF16)

    loads[2].wait()
    loads[3].wait()
    rim_send[...] = gated(length - RIM, RIM, slice(None))
    pl.semaphore_wait(barrier, experts + 2)

    def send_near(k):
        e = near(k)
        return remote(
            near_pack.at[lax.rem(e, NEAR)], arrived.at[ep, pl.ds(mine, 2)],
            sems.at[0, e], sems.at[1, ep], {"ep": e},
        )

    def near_in(s):
        slab = arrived.at[s, pl.ds(mine, 2)]
        return remote(slab, slab, sems.at[0, s], sems.at[1, s], {"ep": s})

    def send_far(j):
        e = far_target(j)
        return remote(
            far_pack.at[e], arrived.at[ep, pos], sems.at[0, e], sems.at[1, ep], {"ep": e}
        )

    def far_in(s):
        slot = arrived.at[s, pos]
        return remote(slot, slot, sems.at[0, s], sems.at[1, s], {"ep": s})

    def xf(s):
        slot = arrived.at[s, pos]
        return remote(slot, slot, sems.at[2, s], sems.at[3, s], xpeer)

    def xf_in(s):
        slot = arrived.at[s, posx]
        return remote(slot, slot, sems.at[2, s], sems.at[3, s], xpeer)

    def cf(s):
        slab = arrived.at[s, pl.ds(mine, 2)]
        return remote(slab, slab, sems.at[4, s], sems.at[5, s], cpeer)

    def cf_in(s):
        slab = arrived.at[s, pl.ds(2 - mine, 2)]
        return remote(slab, slab, sems.at[4, s], sems.at[5, s], cpeer)

    def give_a(s):
        return remote(part.at[s, 1 - core], a_recv.at[s], sems.at[6, s], sems.at[7, s], cpeer)

    def give_b(s):
        return remote(b_send.at[s], b_recv.at[s], sems.at[8, s], sems.at[9, s], xpeer)

    def give_c(s):
        return remote(c_send.at[s], c_recv.at[ep], sems.at[10, s], sems.at[11, ep], {"ep": s})

    def give_c_in(e):
        return remote(c_recv.at[e], c_recv.at[e], sems.at[10, e], sems.at[11, e], {"ep": e})

    after = lax.rem(ep + 1, experts)
    prior = lax.rem(ep + experts - 1, experts)
    rim_out = remote(rim_send, rim_recv, t_sems.at[0, 0], t_sems.at[1, 0], {"ep": after})
    rim_in = remote(rim_recv, rim_recv, t_sems.at[0, 0], t_sems.at[1, 0], {"ep": prior})
    stat_out = [
        remote(stat_send, stat_recv.at[p], t_sems.at[0, p + 1], t_sems.at[1, p + 1], peer)
        for p, peer in enumerate((xpeer, cpeer, dpeer))
    ]
    mix_a = remote(m_part.at[1 - core], m_a, m_sems.at[0], m_sems.at[1], cpeer)
    mix_b = remote(m_bs, m_b, m_sems.at[2], m_sems.at[3], xpeer)

    rim_out.start()
    for k in range(1, NEAR):
        send_near(k).start()
    cf(ep).start()

    @pl.loop(1, groups)
    def _(q):
        other = lax.rem(grp + q, groups)
        pick = selected(0, other)
        for n in range(0, width, tile):
            y = jnp.dot(pick, normed[0, :, n : n + tile], preferred_element_type=F32)
            far_pack[pl.ds(other * NEAR, NEAR), :, n : n + tile] = y.reshape(
                NEAR, cap, tile
            ).astype(BF16)
        for k in range(NEAR):
            send_far((q - 1) * NEAR + k).start()

    strips = chans // LANES

    @pl.loop(0, length // 64)
    def _(r):
        here = pl.multiple_of(r * 64, 64)
        for lane in range(strips):
            at = slice(lane * LANES, (lane + 1) * LANES)
            padded[lane, pl.ds(here + RIM, 64)] = gated(here, 64, at).astype(F32)

    def ffn(s):
        x = joined(arrived[s])
        gate = jnp.minimum(jnp.dot(x, gate_w[...], preferred_element_type=F32), LIMIT)
        lin = jnp.clip(jnp.dot(x, lin_w[...], preferred_element_type=F32), -LIMIT, LIMIT)
        hidden = (gate * jax.nn.sigmoid(SLOPE * gate) * (lin + 1.0)).astype(BF16)
        for n in range(0, width, tile):
            y = jnp.dot(hidden, down_w[:, n : n + tile], preferred_element_type=F32)
            part[s, :, :, :, n : n + tile] = y.reshape(2, 2, cap, tile).astype(BF16)

    def convolve():
        rim_in.wait_recv()
        open_rim = jnp.where(ep > 0, 1.0, 0.0)
        for lane in range(strips):
            padded[lane, 0:RIM] = (
                rim_recv[:, lane * LANES : (lane + 1) * LANES].astype(F32) * open_rim
            )

        @pl.loop(0, length // 64)
        def _(r):
            here = pl.multiple_of(r * 64, 64)
            sums = jnp.zeros((64, LANES), F32)
            squares = jnp.zeros((64, LANES), F32)
            for lane in range(strips):
                value_sum = jnp.zeros((64, LANES), F32)
                for tap in range(taps):
                    value_sum = value_sum + (
                        kern[tap : tap + 1, lane * LANES : (lane + 1) * LANES]
                        * padded[lane, pl.ds(here + (RIM - taps + 1 + tap), 64)]
                    )
                conv[lane, pl.ds(here, 64)] = value_sum
                sums = sums + value_sum
                squares = squares + value_sum * value_sum
            tot[pl.ds(here, 64)] = sums
            squ[pl.ds(here, 64)] = squares

        blocks = length // rows
        for t in range(blocks):
            at = slice(t * rows, (t + 1) * rows)
            stat_send[t : t + 1] = jnp.sum(tot[at].T, axis=0, keepdims=True)
            stat_send[blocks + t : blocks + t + 1] = jnp.sum(squ[at].T, axis=0, keepdims=True)
        for copy in stat_out:
            copy.start()

    def mix():
        for copy in stat_out:
            copy.wait_recv()
        stats = stat_send[...] + stat_recv[0] + stat_recv[1] + stat_recv[2]
        blocks = length // rows
        mean = stats[:blocks] / (chans * 4)
        var = stats[blocks:] / (chans * 4) - mean * mean
        scale = lax.rsqrt(var + EPS)
        for t in range(blocks):
            at = slice(t * rows, (t + 1) * rows)
            middle = jnp.broadcast_to(mean[t : t + 1], (LANES, rows)).T
            spread = jnp.broadcast_to(scale[t : t + 1], (LANES, rows)).T
            for lane in range(strips):
                over = slice(lane * LANES, (lane + 1) * LANES)
                centred = (conv[lane, at] - middle) * spread * ngain[:, over]
                act[at, over] = jax.nn.silu(centred).astype(BF16)
        loads[7].wait()
        for n in range(0, width, tile):
            y = jnp.dot(act[...], proj_w[:, n : n + tile], preferred_element_type=F32)
            for t in range(4):
                m_part[t % 2, t // 2, :, n : n + tile] = y[t * rows : (t + 1) * rows].astype(BF16)
        mix_a.start()

    def due(i, late, step):
        at = i - late

        @pl.when(jnp.logical_and(at >= 0, at < experts))
        def _():
            step(source(at))

    def expert_step(s):
        cf_in(s).wait_recv()
        ffn(s)
        give_a(s).start()

    def first_sum(s):
        give_a(s).wait_recv()
        b_send[s] = (part[s, core, 1 - side].astype(F32) + a_recv[s, 1 - side].astype(F32)).astype(BF16)
        give_b(s).start()

    def second_sum(s):
        give_b(s).wait_recv()
        total = part[s, core, side].astype(F32) + a_recv[s, side].astype(F32) + b_recv[s].astype(F32)

        @pl.when(s == ep)
        def _():
            c_recv[s] = total.astype(BF16)

        @pl.when(s != ep)
        def _():
            c_send[s] = total.astype(BF16)
            give_c(s).start()

    for load in loads[4:7]:
        load.wait()

    def arrival(i, s):
        @pl.when(near_step(i))
        def _():
            near_in(s).wait_recv()
            cf(s).start()

        @pl.when(jnp.logical_not(near_step(i)))
        def _():
            xf_in(s).wait_recv()
            cf(s).start()

    @pl.loop(1, experts + 3)
    def _(i):
        due(i, 1, expert_step)
        due(i, 3, second_sum)
        due(i, 1, first_sum)

        @pl.when(i == 1)
        def _():
            convolve()

        @pl.when(i == 2)
        def _():
            mix()

        @pl.when(i == experts)
        def _():
            mix_a.wait_recv()
            m_bs[...] = (m_part[core, 1 - side].astype(F32) + m_a[1 - side].astype(F32)).astype(BF16)
            mix_b.start()

        @pl.when(i <= experts - NEAR)
        def _():
            s = far_source(i - 1)
            far_in(s).wait_recv()
            xf(s).start()

        due(i, 0, lambda s: arrival(i, s))

    mix_b.wait_recv()
    mix_out[...] = (
        m_part[core, side].astype(F32) + m_a[side].astype(F32) + m_b[...].astype(F32)
    ).astype(BF16)

    order = lax.broadcasted_iota(jnp.int32, (cap, rows), 0).astype(F32)
    per = LANES // cap
    for e in range(0, experts, per):
        stacked = jnp.concatenate(
            [jnp.where(slots[0, e + p] == order, weights[e + p], 0.0) for p in range(per)], axis=0
        ).T
        over = slice(e * cap, e * cap + LANES)
        wmat[:, over] = stacked

    @pl.loop(1, experts)
    def _(d):
        give_c_in(lax.rem(ep + d, experts)).wait_recv()

    weight = wmat[...]
    high = weight.astype(BF16)
    low = (weight - high.astype(F32)).astype(BF16)
    for n in range(0, width, tile):
        results = joined(c_recv[:, :, n : n + tile])
        moe_out[:, n : n + tile] = (
            jnp.dot(high, results, preferred_element_type=F32)
            + jnp.dot(low, results, preferred_element_type=F32)
        ).astype(BF16)

    mix_a.wait_send()
    mix_b.wait_send()
    rim_out.wait_send()
    for copy in stat_out:
        copy.wait_send()
    for k in range(1, NEAR):
        send_near(k).wait_send()

    @pl.loop(0, experts - NEAR)
    def _(j):
        send_far(j).wait_send()
        xf(far_source(j)).wait_send()

    @pl.loop(0, experts)
    def _(s):
        @pl.when(s != ep)
        def _():
            give_c(s).wait_send()

        cf(s).wait_send()
        give_a(s).wait_send()
        give_b(s).wait_send()


def shards(
    conv_value,
    conv_gate,
    conv_kernel,
    norm_gain,
    mixer_proj,
    moe_in,
    route_ids,
    route_logits,
    moe_gain,
    expert_gate,
    expert_lin,
    expert_down,
):
    tp_size = lax.axis_size("tp")
    experts = lax.axis_size("ep")
    tokens, width = moe_in.shape
    rows = tokens // tp_size
    topk = route_ids.shape[1]
    capacity = max(2, 2 * rows * topk // experts)
    hid = expert_gate.shape[2]
    length, chans = conv_value.shape
    padded_experts = -(-experts // 8) * 8
    if tp_size != 4 or experts % NEAR or topk != 2 or length != tokens or rows != LANES:
        raise ValueError("unsupported sizes")

    def by_block(table):
        return table.reshape(tp_size, rows, topk).transpose(0, 2, 1)

    vmem = pl.BlockSpec(memory_space=pltpu.VMEM)
    hbm = pl.BlockSpec(memory_space=pl.ANY)
    out = jax.ShapeDtypeStruct((rows, width), BF16)
    slot_rows = (experts, capacity, width)
    mixer_out, moe_out = pl.pallas_call(
        layer_kernel,
        out_shape=(out, out),
        in_specs=[vmem] * 5 + [hbm] * 7,
        out_specs=(vmem, vmem),
        scratch_shapes=[
            pltpu.VMEM((width, hid), BF16),
            pltpu.VMEM((width, hid), BF16),
            pltpu.VMEM((hid, width), BF16),
            pltpu.VMEM((chans, width), BF16),
            pltpu.VMEM((2, rows, width), BF16),
            pltpu.VMEM((2, rows, width), BF16),
            pltpu.VMEM((2, padded_experts, 1, rows), F32),
            pltpu.VMEM((padded_experts, 1, rows), F32),
            pltpu.VMEM(slot_rows, BF16),
            pltpu.VMEM((NEAR, 2, capacity, width), BF16),
            pltpu.VMEM((experts, tp_size, capacity, width), BF16),
            pltpu.VMEM((experts, 2, 2, capacity, width), BF16),
            pltpu.VMEM((experts, 2, capacity, width), BF16),
            pltpu.VMEM(slot_rows, BF16),
            pltpu.VMEM(slot_rows, BF16),
            pltpu.VMEM(slot_rows, BF16),
            pltpu.VMEM(slot_rows, BF16),
            pltpu.VMEM((length, chans), BF16),
            pltpu.VMEM((length, chans), BF16),
            pltpu.VMEM((chans // LANES, length + RIM, LANES), F32),
            pltpu.VMEM((chans // LANES, length, LANES), F32),
            pltpu.VMEM((length, LANES), F32),
            pltpu.VMEM((length, LANES), F32),
            pltpu.VMEM((length, chans), BF16),
            pltpu.VMEM((RIM, chans), BF16),
            pltpu.VMEM((RIM, chans), BF16),
            pltpu.VMEM((8, LANES), F32),
            pltpu.VMEM((3, 8, LANES), F32),
            pltpu.VMEM((2, 2, rows, width), BF16),
            pltpu.VMEM((2, rows, width), BF16),
            pltpu.VMEM((rows, width), BF16),
            pltpu.VMEM((rows, width), BF16),
            pltpu.VMEM((rows, experts * capacity), F32),
            pltpu.SemaphoreType.DMA((8,)),
            pltpu.SemaphoreType.DMA((12, experts)),
            pltpu.SemaphoreType.DMA((2, 4)),
            pltpu.SemaphoreType.DMA((4,)),
        ],
        compiler_params=pltpu.CompilerParams(
            has_side_effects=True, collective_id=0, vmem_limit_bytes=62 * 1024 * 1024
        ),
    )(
        by_block(route_ids), by_block(route_logits), conv_kernel, norm_gain[None], moe_gain[None],
        moe_in, conv_value, conv_gate, expert_gate[0], expert_lin[0], expert_down[0], mixer_proj,
    )
    return (mixer_out, moe_out)


def solution(mesh):
    placed = (
        P("ep", "tp"),
        P("ep", "tp"),
        P(None, "tp"),
        P("tp"),
        P("tp", None),
        P("ep", None),
        P("ep", None),
        P("ep", None),
        P(),
        P("ep", None, "tp"),
        P("ep", None, "tp"),
        P("ep", "tp", None),
    )
    return jax.shard_map(
        shards,
        mesh=mesh,
        in_specs=placed,
        out_specs=(P(("ep", "tp"), None), P(("ep", "tp"), None)),
        check_vma=False,
    )
```

```python
import jax
import jax.numpy as jnp
from jax import lax
from jax.experimental import pallas as pl
from jax.experimental.pallas import tpu as pltpu
from jax.sharding import PartitionSpec as P

EPS = 1e-05
LIMIT = 7.0
SLOPE = 1.702
F32 = jnp.float32
BF16 = jnp.bfloat16
LANES = 128
RIM = 32
NEAR = 4


def remote(src, dst, send, recv, device):
    return pltpu.make_async_remote_copy(
        src_ref=src,
        dst_ref=dst,
        send_sem=send,
        recv_sem=recv,
        device_id=device,
        device_id_type=pl.DeviceIdType.MESH,
    )


def joined(block):
    groups, rows, width = block.shape
    if rows % 16:
        return block.astype(F32).reshape(groups * rows, width).astype(BF16)
    return block.reshape(groups * rows, width)


def layer_kernel(
    ids, logits, kern, ngain, mgain,
    moe_hbm, value_hbm, cgate_hbm, gate_hbm, lin_hbm, down_hbm, proj_hbm,
    mix_out, moe_out,
    gate_w, lin_w, down_w, proj_w,
    xrows, normed, slots, weights, far_pack, near_pack, tokens, table,
    arrived, part, a_recv, b_send, b_recv, c_send, c_recv,
    value, cgate, padded, conv, tot, squ, act, rim_send, rim_recv, stat_send, stat_recv,
    m_part, m_a, m_bs, m_b,
    wmat, load_sem, sems, t_sems, m_sems, g_sems,
):
    experts, _, cap, width = arrived.shape
    rows = moe_out.shape[0]
    length, chans = value.shape
    taps = kern.shape[0]
    groups = experts // NEAR
    ep, tp = lax.axis_index("ep"), lax.axis_index("tp")
    core, side = lax.rem(tp, 2), lax.div(tp, 2)
    xpeer, cpeer = {"tp": lax.rem(tp + 2, 4)}, {"tp": tp + 1 - 2 * core}
    dpeer = {"tp": lax.rem(tp + 3 - 2 * core, 4)}
    pos, posx = core * 2 + side, core * 2 + 1 - side
    mine = core * 2
    grp = lax.div(ep, NEAR)
    mem = lax.rem(ep, NEAR)
    row, col = lax.div(mem, 2), lax.rem(mem, 2)
    mirror = (1 - row) * 2 + col

    def near(k):
        return grp * NEAR + lax.rem(row + k // 2, 2) * 2 + lax.rem(col + k, 2)

    def far_source(j):
        other = lax.rem(grp + lax.div(j, NEAR) + 1, groups)
        k = lax.rem(j, NEAR)
        return other * NEAR + lax.rem(row + 1 + lax.div(k, 2), 2) * 2 + lax.rem(col + k, 2)

    def near_step(i):
        return jnp.logical_or(i < 3, i == experts - 1)

    def source(i):
        k = jnp.minimum(i, 3)
        close = grp * NEAR + lax.rem(row + lax.div(k, 2), 2) * 2 + lax.rem(col + k, 2)
        distant = far_source(jnp.clip(i - 3, 0, experts - NEAR - 1))
        return jnp.where(near_step(i), close, distant)

    loads = [
        pltpu.make_async_copy(moe_hbm.at[pl.ds(tp * rows, rows)], xrows.at[0], load_sem.at[0]),
        pltpu.make_async_copy(
            moe_hbm.at[pl.ds(lax.rem(tp + 2, 4) * rows, rows)], xrows.at[1], load_sem.at[1]
        ),
        pltpu.make_async_copy(value_hbm, value, load_sem.at[2]),
        pltpu.make_async_copy(cgate_hbm, cgate, load_sem.at[3]),
        pltpu.make_async_copy(gate_hbm, gate_w, load_sem.at[4]),
        pltpu.make_async_copy(lin_hbm, lin_w, load_sem.at[5]),
        pltpu.make_async_copy(down_hbm, down_w, load_sem.at[6]),
        pltpu.make_async_copy(proj_hbm, proj_w, load_sem.at[7]),
    ]
    for load in loads:
        load.start()

    barrier = pltpu.get_barrier_semaphore()

    @pl.loop(1, experts)
    def _(d):
        pl.semaphore_signal(
            barrier, inc=1, device_id={"ep": lax.rem(ep + d, experts)},
            device_id_type=pl.DeviceIdType.MESH,
        )

    for peer in (xpeer, cpeer, dpeer):
        pl.semaphore_signal(barrier, inc=1, device_id=peer, device_id_type=pl.DeviceIdType.MESH)

    padded_experts = -(-experts // 8) * 8
    before = (
        lax.broadcasted_iota(jnp.int32, (rows, rows), 0)
        < lax.broadcasted_iota(jnp.int32, (rows, rows), 1)
    ).astype(BF16)
    names = lax.broadcasted_iota(jnp.int32, (padded_experts, rows), 0)
    for b, block in ((0, tp), (1, lax.rem(tp + 2, 4))):
        chosen = ids[block]
        first, second = chosen[0:1] == names, chosen[1:2] == names
        taken = jnp.where(jnp.logical_or(first, second), 1.0, 0.0)
        rank = jnp.dot(taken.astype(BF16), before, preferred_element_type=F32)
        place = jnp.where(taken > 0.0, rank, -1.0)
        for e in range(experts):
            slots[b, e] = place[e : e + 1]
        if b == 0:
            expo = jnp.exp(logits[block])
            total = expo[0:1] + expo[1:2]
            share = jnp.where(first, expo[0:1] / total, 0.0) + jnp.where(
                second, expo[1:2] / total, 0.0
            )
            for e in range(experts):
                weights[e] = share[e : e + 1]

    def selected(places):
        order = lax.broadcasted_iota(jnp.int32, (cap, rows), 0).astype(F32)
        picks = [jnp.where(place == order, 1.0, 0.0) for place in places]
        return jnp.concatenate(picks, axis=0).astype(BF16)

    for b in range(2):
        loads[b].wait()
        for r in range(0, rows, 16):
            block = xrows[b, r : r + 16].astype(F32)
            mu = jnp.mean(block, axis=1, keepdims=True)
            block = block - mu
            va = jnp.mean(jnp.square(block), axis=1, keepdims=True)
            normed[b, r : r + 16] = (block * lax.rsqrt(va + EPS) * mgain[...]).astype(BF16)

    tile = min(512, width)
    def gated(start, count, over):
        glu = value[pl.ds(start, count), over].astype(F32) * jax.nn.sigmoid(
            cgate[pl.ds(start, count), over].astype(F32)
        )
        return glu.astype(BF16)

    loads[2].wait()
    loads[3].wait()
    rim_send[...] = gated(length - RIM, RIM, slice(None))

    def send_near(k):
        e = near(k)
        return remote(
            near_pack.at[lax.rem(e, NEAR)], arrived.at[ep, pl.ds(mine, 2)],
            sems.at[0, e], sems.at[1, ep], {"ep": e},
        )

    def near_in(s):
        slab = arrived.at[s, pl.ds(mine, 2)]
        return remote(slab, slab, sems.at[0, s], sems.at[1, s], {"ep": s})

    def send_tokens(q):
        other = lax.rem(grp + q, groups)
        return remote(
            normed.at[0], tokens.at[grp], g_sems.at[0, other], g_sems.at[1, grp],
            {"ep": other * NEAR + mirror},
        )

    def tokens_in(other):
        return remote(
            tokens.at[other], tokens.at[other], g_sems.at[0, other], g_sems.at[1, other], {"ep": other * NEAR + mirror}
        )

    def send_table(q):
        other = lax.rem(grp + q, groups)
        return remote(
            slots.at[0, pl.ds(other * NEAR, NEAR)], table.at[grp],
            g_sems.at[2, other], g_sems.at[3, grp], {"ep": other * NEAR + mirror},
        )

    def table_in(other):
        return remote(
            table.at[other], table.at[other], g_sems.at[2, other], g_sems.at[3, other], {"ep": other * NEAR + mirror}
        )

    def send_relayed(other, k):
        e = near(k)
        place = other * NEAR + lax.rem(e, NEAR)
        return remote(
            far_pack.at[place], arrived.at[other * NEAR + mirror, pos],
            sems.at[0, place], sems.at[1, other * NEAR + mirror], {"ep": e},
        )

    def relay(other):
        tokens_in(other).wait_recv()
        table_in(other).wait_recv()
        pick = selected([table[other, m] for m in range(NEAR)])
        for n in range(0, width, tile):
            y = jnp.dot(pick, tokens[other, :, n : n + tile], preferred_element_type=F32)
            far_pack[pl.ds(other * NEAR, NEAR), :, n : n + tile] = y.reshape(
                NEAR, cap, tile
            ).astype(BF16)
        for k in range(1, NEAR):
            send_relayed(other, k).start()
        arrived[other * NEAR + mirror, pos] = far_pack[other * NEAR + mem]

    def far_in(s):
        slot = arrived.at[s, pos]
        return remote(slot, slot, sems.at[0, s], sems.at[1, s], {"ep": s})

    def xf(s):
        slot = arrived.at[s, pos]
        return remote(slot, slot, sems.at[2, s], sems.at[3, s], xpeer)

    def xf_in(s):
        slot = arrived.at[s, posx]
        return remote(slot, slot, sems.at[2, s], sems.at[3, s], xpeer)

    def cf(s):
        slab = arrived.at[s, pl.ds(mine, 2)]
        return remote(slab, slab, sems.at[4, s], sems.at[5, s], cpeer)

    def cf_in(s):
        slab = arrived.at[s, pl.ds(2 - mine, 2)]
        return remote(slab, slab, sems.at[4, s], sems.at[5, s], cpeer)

    def give_a(s):
        return remote(part.at[s, 1 - core], a_recv.at[s], sems.at[6, s], sems.at[7, s], cpeer)

    def give_b(s):
        return remote(b_send.at[s], b_recv.at[s], sems.at[8, s], sems.at[9, s], xpeer)

    def give_c(s):
        return remote(c_send.at[s], c_recv.at[ep], sems.at[10, s], sems.at[11, ep], {"ep": s})

    def give_c_in(e):
        return remote(c_recv.at[e], c_recv.at[e], sems.at[10, e], sems.at[11, e], {"ep": e})

    after = lax.rem(ep + 1, experts)
    prior = lax.rem(ep + experts - 1, experts)
    rim_out = remote(rim_send, rim_recv, t_sems.at[0, 0], t_sems.at[1, 0], {"ep": after})
    rim_in = remote(rim_recv, rim_recv, t_sems.at[0, 0], t_sems.at[1, 0], {"ep": prior})
    stat_out = [
        remote(stat_send, stat_recv.at[p], t_sems.at[0, p + 1], t_sems.at[1, p + 1], peer)
        for p, peer in enumerate((xpeer, cpeer, dpeer))
    ]
    mix_a = remote(m_part.at[1 - core], m_a, m_sems.at[0, 0], m_sems.at[1, 0], cpeer)
    half = rows // 2
    mix_b = [
        remote(
            m_bs.at[pl.ds(h * half, half)], m_b.at[pl.ds(h * half, half)],
            m_sems.at[2, h], m_sems.at[3, h], xpeer,
        )
        for h in range(2)
    ]

    pl.semaphore_wait(barrier, experts + 2)
    rim_out.start()

    @pl.loop(1, groups)
    def _(q):
        send_table(q).start()

    for b in range(2):
        pick = selected([slots[b, grp * NEAR + m] for m in range(NEAR)])
        where = side if b == 0 else 1 - side
        for n in range(0, width, tile):
            y = jnp.dot(pick, normed[b, :, n : n + tile], preferred_element_type=F32)
            near_pack[:, where, :, n : n + tile] = y.reshape(NEAR, cap, tile).astype(BF16)

    arrived[ep, pl.ds(mine, 2)] = near_pack[mem]
    send_near(1).start()
    cf(ep).start()

    @pl.loop(1, groups)
    def _(q):
        send_tokens(q).start()

    send_near(2).start()

    strips = chans // LANES

    @pl.loop(0, length // 64)
    def _(r):
        here = pl.multiple_of(r * 64, 64)
        for lane in range(strips):
            at = slice(lane * LANES, (lane + 1) * LANES)
            padded[lane, pl.ds(here + RIM, 64)] = gated(here, 64, at).astype(F32)

    def ffn(s):
        x = joined(arrived[s])
        gate = jnp.minimum(jnp.dot(x, gate_w[...], preferred_element_type=F32), LIMIT)
        lin = jnp.clip(jnp.dot(x, lin_w[...], preferred_element_type=F32), -LIMIT, LIMIT)
        hidden = (gate * jax.nn.sigmoid(SLOPE * gate) * (lin + 1.0)).astype(BF16)
        for n in range(0, width, tile):
            y = jnp.dot(hidden, down_w[:, n : n + tile], preferred_element_type=F32)
            part[s, :, :, :, n : n + tile] = y.reshape(2, 2, cap, tile).astype(BF16)

    def convolve():
        rim_in.wait_recv()
        open_rim = jnp.where(ep > 0, 1.0, 0.0)
        for lane in range(strips):
            padded[lane, 0:RIM] = (
                rim_recv[:, lane * LANES : (lane + 1) * LANES].astype(F32) * open_rim
            )

        @pl.loop(0, length // 64)
        def _(r):
            here = pl.multiple_of(r * 64, 64)
            sums = jnp.zeros((64, LANES), F32)
            squares = jnp.zeros((64, LANES), F32)
            for lane in range(strips):
                value_sum = jnp.zeros((64, LANES), F32)
                for tap in range(taps):
                    value_sum = value_sum + (
                        kern[tap : tap + 1, lane * LANES : (lane + 1) * LANES]
                        * padded[lane, pl.ds(here + (RIM - taps + 1 + tap), 64)]
                    )
                conv[lane, pl.ds(here, 64)] = value_sum
                sums = sums + value_sum
                squares = squares + value_sum * value_sum
            tot[pl.ds(here, 64)] = sums
            squ[pl.ds(here, 64)] = squares

        blocks = length // rows
        for t in range(blocks):
            at = slice(t * rows, (t + 1) * rows)
            stat_send[t : t + 1] = jnp.sum(tot[at].T, axis=0, keepdims=True)
            stat_send[blocks + t : blocks + t + 1] = jnp.sum(squ[at].T, axis=0, keepdims=True)
        for copy in stat_out:
            copy.start()

    def mix():
        for copy in stat_out:
            copy.wait_recv()
        stats = stat_send[...] + stat_recv[0] + stat_recv[1] + stat_recv[2]
        blocks = length // rows
        mean = stats[:blocks] / (chans * 4)
        var = stats[blocks:] / (chans * 4) - mean * mean
        scale = lax.rsqrt(var + EPS)
        for t in range(blocks):
            at = slice(t * rows, (t + 1) * rows)
            middle = jnp.broadcast_to(mean[t : t + 1], (LANES, rows)).T
            spread = jnp.broadcast_to(scale[t : t + 1], (LANES, rows)).T
            for lane in range(strips):
                over = slice(lane * LANES, (lane + 1) * LANES)
                centred = (conv[lane, at] - middle) * spread * ngain[:, over]
                act[at, over] = jax.nn.silu(centred).astype(BF16)
        loads[7].wait()
        for n in range(0, width, tile):
            y = jnp.dot(act[...], proj_w[:, n : n + tile], preferred_element_type=F32)
            for t in range(4):
                m_part[t % 2, t // 2, :, n : n + tile] = y[t * rows : (t + 1) * rows].astype(BF16)
        mix_a.start()

    def due(i, late, step):
        at = i - late

        @pl.when(jnp.logical_and(at >= 0, at < experts))
        def _():
            step(source(at))

    def expert_step(s):
        cf_in(s).wait_recv()
        ffn(s)
        give_a(s).start()

    def first_sum(s):
        give_a(s).wait_recv()
        b_send[s] = (part[s, core, 1 - side].astype(F32) + a_recv[s, 1 - side].astype(F32)).astype(BF16)
        give_b(s).start()

    def second_sum(s):
        give_b(s).wait_recv()
        total = part[s, core, side].astype(F32) + a_recv[s, side].astype(F32) + b_recv[s].astype(F32)

        @pl.when(s == ep)
        def _():
            c_recv[s] = total.astype(BF16)

        @pl.when(s != ep)
        def _():
            c_send[s] = total.astype(BF16)
            give_c(s).start()

    convolve()
    for load in loads[4:7]:
        load.wait()

    def arrival(i, s):
        @pl.when(near_step(i))
        def _():
            near_in(s).wait_recv()
            cf(s).start()

        @pl.when(jnp.logical_not(near_step(i)))
        def _():
            xf_in(s).wait_recv()
            cf(s).start()

    @pl.loop(1, experts + 2)
    def _(i):
        @pl.when(i == 2)
        def _():
            mix_a.wait_recv()
            m_bs[...] = (m_part[core, 1 - side].astype(F32) + m_a[1 - side].astype(F32)).astype(BF16)
            mix_b[0].start()

        due(i, 1, expert_step)
        due(i, 1, first_sum)

        @pl.when(i == 1)
        def _():
            mix()

        @pl.when(i == 2)
        def _():
            @pl.loop(1, groups)
            def _(q):
                relay(lax.rem(grp + q, groups))

        @pl.when(jnp.logical_and(i > 1, i < experts - 2))
        def _():
            j = i - 2
            s = far_source(j)

            @pl.when(lax.rem(j, NEAR) > 0)
            def _():
                far_in(s).wait_recv()

            xf(s).start()

        @pl.when(i == 4)
        def _():
            send_near(3).start()

        @pl.when(i == experts)
        def _():
            mix_b[1].start()

        due(i, 2, second_sum)
        due(i, 0, lambda s: arrival(i, s))

    for copy in mix_b:
        copy.wait_recv()
    mix_out[...] = (
        m_part[core, side].astype(F32) + m_a[side].astype(F32) + m_b[...].astype(F32)
    ).astype(BF16)

    order = lax.broadcasted_iota(jnp.int32, (cap, rows), 0).astype(F32)
    per = LANES // cap
    for e in range(0, experts, per):
        stacked = jnp.concatenate(
            [jnp.where(slots[0, e + p] == order, weights[e + p], 0.0) for p in range(per)], axis=0
        ).T
        over = slice(e * cap, e * cap + LANES)
        wmat[:, over] = stacked

    @pl.loop(1, experts)
    def _(d):
        give_c_in(lax.rem(ep + d, experts)).wait_recv()

    weight = wmat[...]
    high = weight.astype(BF16)
    low = (weight - high.astype(F32)).astype(BF16)
    for n in range(0, width, tile):
        results = joined(c_recv[:, :, n : n + tile])
        moe_out[:, n : n + tile] = (
            jnp.dot(high, results, preferred_element_type=F32)
            + jnp.dot(low, results, preferred_element_type=F32)
        ).astype(BF16)

    mix_a.wait_send()
    for copy in mix_b:
        copy.wait_send()
    rim_out.wait_send()
    for copy in stat_out:
        copy.wait_send()
    for k in range(1, NEAR):
        send_near(k).wait_send()

    @pl.loop(1, groups)
    def _(q):
        send_table(q).wait_send()
        send_tokens(q).wait_send()
        for k in range(1, NEAR):
            send_relayed(lax.rem(grp + q, groups), k).wait_send()

    @pl.loop(0, experts - NEAR)
    def _(j):
        xf(far_source(j)).wait_send()

    @pl.loop(0, experts)
    def _(s):
        @pl.when(s != ep)
        def _():
            give_c(s).wait_send()

        cf(s).wait_send()
        give_a(s).wait_send()
        give_b(s).wait_send()


def shards(
    conv_value,
    conv_gate,
    conv_kernel,
    norm_gain,
    mixer_proj,
    moe_in,
    route_ids,
    route_logits,
    moe_gain,
    expert_gate,
    expert_lin,
    expert_down,
):
    tp_size = lax.axis_size("tp")
    experts = lax.axis_size("ep")
    tokens, width = moe_in.shape
    rows = tokens // tp_size
    topk = route_ids.shape[1]
    capacity = max(2, 2 * rows * topk // experts)
    hid = expert_gate.shape[2]
    length, chans = conv_value.shape
    padded_experts = -(-experts // 8) * 8
    if tp_size != 4 or experts % NEAR or topk != 2 or length != tokens or rows != LANES:
        raise ValueError("unsupported sizes")

    def by_block(table):
        return table.reshape(tp_size, rows, topk).transpose(0, 2, 1)

    vmem = pl.BlockSpec(memory_space=pltpu.VMEM)
    hbm = pl.BlockSpec(memory_space=pl.ANY)
    out = jax.ShapeDtypeStruct((rows, width), BF16)
    slot_rows = (experts, capacity, width)
    mixer_out, moe_out = pl.pallas_call(
        layer_kernel,
        out_shape=(out, out),
        in_specs=[vmem] * 5 + [hbm] * 7,
        out_specs=(vmem, vmem),
        scratch_shapes=[
            pltpu.VMEM((width, hid), BF16),
            pltpu.VMEM((width, hid), BF16),
            pltpu.VMEM((hid, width), BF16),
            pltpu.VMEM((chans, width), BF16),
            pltpu.VMEM((2, rows, width), BF16),
            pltpu.VMEM((2, rows, width), BF16),
            pltpu.VMEM((2, padded_experts, 1, rows), F32),
            pltpu.VMEM((padded_experts, 1, rows), F32),
            pltpu.VMEM(slot_rows, BF16),
            pltpu.VMEM((NEAR, 2, capacity, width), BF16),
            pltpu.VMEM((experts // NEAR, rows, width), BF16),
            pltpu.VMEM((experts // NEAR, NEAR, 1, rows), F32),
            pltpu.VMEM((experts, tp_size, capacity, width), BF16),
            pltpu.VMEM((experts, 2, 2, capacity, width), BF16),
            pltpu.VMEM((experts, 2, capacity, width), BF16),
            pltpu.VMEM(slot_rows, BF16),
            pltpu.VMEM(slot_rows, BF16),
            pltpu.VMEM(slot_rows, BF16),
            pltpu.VMEM(slot_rows, BF16),
            pltpu.VMEM((length, chans), BF16),
            pltpu.VMEM((length, chans), BF16),
            pltpu.VMEM((chans // LANES, length + RIM, LANES), F32),
            pltpu.VMEM((chans // LANES, length, LANES), F32),
            pltpu.VMEM((length, LANES), F32),
            pltpu.VMEM((length, LANES), F32),
            pltpu.VMEM((length, chans), BF16),
            pltpu.VMEM((RIM, chans), BF16),
            pltpu.VMEM((RIM, chans), BF16),
            pltpu.VMEM((8, LANES), F32),
            pltpu.VMEM((3, 8, LANES), F32),
            pltpu.VMEM((2, 2, rows, width), BF16),
            pltpu.VMEM((2, rows, width), BF16),
            pltpu.VMEM((rows, width), BF16),
            pltpu.VMEM((rows, width), BF16),
            pltpu.VMEM((rows, experts * capacity), F32),
            pltpu.SemaphoreType.DMA((8,)),
            pltpu.SemaphoreType.DMA((12, experts)),
            pltpu.SemaphoreType.DMA((2, 4)),
            pltpu.SemaphoreType.DMA((4, 2)),
            pltpu.SemaphoreType.DMA((4, experts // NEAR)),
        ],
        compiler_params=pltpu.CompilerParams(
            has_side_effects=True, collective_id=0, vmem_limit_bytes=62 * 1024 * 1024
        ),
    )(
        by_block(route_ids), by_block(route_logits), conv_kernel, norm_gain[None], moe_gain[None],
        moe_in, conv_value, conv_gate, expert_gate[0], expert_lin[0], expert_down[0], mixer_proj,
    )
    return (mixer_out, moe_out)


def solution(mesh):
    placed = (
        P("ep", "tp"),
        P("ep", "tp"),
        P(None, "tp"),
        P("tp"),
        P("tp", None),
        P("ep", None),
        P("ep", None),
        P("ep", None),
        P(),
        P("ep", None, "tp"),
        P("ep", None, "tp"),
        P("ep", "tp", None),
    )
    return jax.shard_map(
        shards,
        mesh=mesh,
        in_specs=placed,
        out_specs=(P(("ep", "tp"), None), P(("ep", "tp"), None)),
        check_vma=False,
    )
```

```python
import jax
import jax.numpy as jnp
from jax import lax
from jax.experimental import pallas as pl
from jax.experimental.pallas import tpu as pltpu
from jax.sharding import PartitionSpec as P

EPS = 1e-05
LIMIT = 7.0
SLOPE = 1.702
F32 = jnp.float32
BF16 = jnp.bfloat16
LANES = 128
RIM = 32
NEAR = 4


def remote(src, dst, send, recv, device):
    return pltpu.make_async_remote_copy(
        src_ref=src,
        dst_ref=dst,
        send_sem=send,
        recv_sem=recv,
        device_id=device,
        device_id_type=pl.DeviceIdType.MESH,
    )


def joined(block):
    groups, rows, width = block.shape
    if rows % 16:
        return block.astype(F32).reshape(groups * rows, width).astype(BF16)
    return block.reshape(groups * rows, width)


def layer_kernel(
    ids, logits, kern, ngain, mgain,
    moe_hbm, value_hbm, cgate_hbm, gate_hbm, lin_hbm, down_hbm, proj_hbm,
    mix_out, moe_out,
    gate_w, lin_w, down_w, proj_w,
    xrows, normed, slots, weights, far_pack, near_pack, tokens, table,
    arrived, part, a_recv, b_send, b_recv, c_send, c_recv,
    value, cgate, padded, conv, tot, squ, act, rim_send, rim_recv, stat_send, stat_recv,
    m_part, m_a, m_bs, m_b,
    wmat, summed, load_sem, sems, t_sems, m_sems, g_sems,
):
    experts, _, cap, width = arrived.shape
    rows = moe_out.shape[0]
    length, chans = value.shape
    taps = kern.shape[0]
    groups = experts // NEAR
    ep, tp = lax.axis_index("ep"), lax.axis_index("tp")
    core, side = lax.rem(tp, 2), lax.div(tp, 2)
    xpeer, cpeer = {"tp": lax.rem(tp + 2, 4)}, {"tp": tp + 1 - 2 * core}
    dpeer = {"tp": lax.rem(tp + 3 - 2 * core, 4)}
    pos, posx = core * 2 + side, core * 2 + 1 - side
    mine = core * 2
    grp = lax.div(ep, NEAR)
    mem = lax.rem(ep, NEAR)
    row, col = lax.div(mem, 2), lax.rem(mem, 2)
    mirror = (1 - row) * 2 + col

    def near(k):
        return grp * NEAR + lax.rem(row + k // 2, 2) * 2 + lax.rem(col + k, 2)

    def far_source(j):
        other = lax.rem(grp + lax.div(j, NEAR) + 1, groups)
        k = lax.rem(j, NEAR)
        return other * NEAR + lax.rem(row + 1 + lax.div(k, 2), 2) * 2 + lax.rem(col + k, 2)

    def near_step(i):
        return jnp.logical_or(i < 3, i == experts - 2)

    def source(i):
        k = jnp.minimum(i, 3)
        close = grp * NEAR + lax.rem(row + lax.div(k, 2), 2) * 2 + lax.rem(col + k, 2)
        distant = far_source(jnp.where(i == experts - 1, i - NEAR, jnp.maximum(i - 3, 0)))
        return jnp.where(near_step(i), close, distant)

    loads = [
        pltpu.make_async_copy(moe_hbm.at[pl.ds(tp * rows, rows)], xrows.at[0], load_sem.at[0]),
        pltpu.make_async_copy(
            moe_hbm.at[pl.ds(lax.rem(tp + 2, 4) * rows, rows)], xrows.at[1], load_sem.at[1]
        ),
        pltpu.make_async_copy(value_hbm, value, load_sem.at[2]),
        pltpu.make_async_copy(cgate_hbm, cgate, load_sem.at[3]),
        pltpu.make_async_copy(gate_hbm, gate_w, load_sem.at[4]),
        pltpu.make_async_copy(lin_hbm, lin_w, load_sem.at[5]),
        pltpu.make_async_copy(down_hbm, down_w, load_sem.at[6]),
        pltpu.make_async_copy(proj_hbm, proj_w, load_sem.at[7]),
    ]
    for load in loads:
        load.start()

    barrier = pltpu.get_barrier_semaphore()

    @pl.loop(1, experts)
    def _(d):
        pl.semaphore_signal(
            barrier, inc=1, device_id={"ep": lax.rem(ep + d, experts)},
            device_id_type=pl.DeviceIdType.MESH,
        )

    for peer in (xpeer, cpeer, dpeer):
        pl.semaphore_signal(barrier, inc=1, device_id=peer, device_id_type=pl.DeviceIdType.MESH)

    padded_experts = -(-experts // 8) * 8
    before = (
        lax.broadcasted_iota(jnp.int32, (rows, rows), 0)
        < lax.broadcasted_iota(jnp.int32, (rows, rows), 1)
    ).astype(BF16)
    names = lax.broadcasted_iota(jnp.int32, (padded_experts, rows), 0)
    for b, block in ((0, tp), (1, lax.rem(tp + 2, 4))):
        chosen = ids[block]
        first, second = chosen[0:1] == names, chosen[1:2] == names
        taken = jnp.where(jnp.logical_or(first, second), 1.0, 0.0)
        rank = jnp.dot(taken.astype(BF16), before, preferred_element_type=F32)
        place = jnp.where(taken > 0.0, rank, -1.0)
        for e in range(experts):
            slots[b, e] = place[e : e + 1]
        if b == 0:
            expo = jnp.exp(logits[block])
            total = expo[0:1] + expo[1:2]
            share = jnp.where(first, expo[0:1] / total, 0.0) + jnp.where(
                second, expo[1:2] / total, 0.0
            )
            for e in range(experts):
                weights[e] = share[e : e + 1]

    def selected(places):
        order = lax.broadcasted_iota(jnp.int32, (cap, rows), 0).astype(F32)
        picks = [jnp.where(place == order, 1.0, 0.0) for place in places]
        return jnp.concatenate(picks, axis=0).astype(BF16)

    for b in range(2):
        loads[b].wait()
        for r in range(0, rows, 16):
            block = xrows[b, r : r + 16].astype(F32)
            mu = jnp.mean(block, axis=1, keepdims=True)
            block = block - mu
            va = jnp.mean(jnp.square(block), axis=1, keepdims=True)
            normed[b, r : r + 16] = (block * lax.rsqrt(va + EPS) * mgain[...]).astype(BF16)

    tile = min(512, width)
    def gated(start, count, over):
        glu = value[pl.ds(start, count), over].astype(F32) * jax.nn.sigmoid(
            cgate[pl.ds(start, count), over].astype(F32)
        )
        return glu.astype(BF16)

    loads[2].wait()
    loads[3].wait()
    rim_send[...] = gated(length - RIM, RIM, slice(None))

    def send_near(k):
        e = near(k)
        return remote(
            near_pack.at[lax.rem(e, NEAR)], arrived.at[ep, pl.ds(mine, 2)],
            sems.at[0, e], sems.at[1, ep], {"ep": e},
        )

    def near_in(s):
        slab = arrived.at[s, pl.ds(mine, 2)]
        return remote(slab, slab, sems.at[0, s], sems.at[1, s], {"ep": s})

    def send_tokens(q):
        other = lax.rem(grp + q, groups)
        return remote(
            normed.at[0], tokens.at[grp], g_sems.at[0, other], g_sems.at[1, grp],
            {"ep": other * NEAR + mirror},
        )

    def tokens_in(other):
        return remote(
            tokens.at[other], tokens.at[other], g_sems.at[0, other], g_sems.at[1, other], {"ep": other * NEAR + mirror}
        )

    def send_table(q):
        other = lax.rem(grp + q, groups)
        return remote(
            slots.at[0, pl.ds(other * NEAR, NEAR)], table.at[grp],
            g_sems.at[2, other], g_sems.at[3, grp], {"ep": other * NEAR + mirror},
        )

    def table_in(other):
        return remote(
            table.at[other], table.at[other], g_sems.at[2, other], g_sems.at[3, other], {"ep": other * NEAR + mirror}
        )

    def send_relayed(other, k):
        e = near(k)
        place = other * NEAR + lax.rem(e, NEAR)
        return remote(
            far_pack.at[place], arrived.at[other * NEAR + mirror, pos],
            sems.at[0, place], sems.at[1, other * NEAR + mirror], {"ep": e},
        )

    def relay(other):
        tokens_in(other).wait_recv()
        table_in(other).wait_recv()
        pick = selected([table[other, m] for m in range(NEAR)])
        for n in range(0, width, tile):
            y = jnp.dot(pick, tokens[other, :, n : n + tile], preferred_element_type=F32)
            far_pack[pl.ds(other * NEAR, NEAR), :, n : n + tile] = y.reshape(
                NEAR, cap, tile
            ).astype(BF16)
        for k in range(1, NEAR):
            send_relayed(other, k).start()
        arrived[other * NEAR + mirror, pos] = far_pack[other * NEAR + mem]

    def far_in(s):
        slot = arrived.at[s, pos]
        return remote(slot, slot, sems.at[0, s], sems.at[1, s], {"ep": s})

    def xf(s):
        slot = arrived.at[s, pos]
        return remote(slot, slot, sems.at[2, s], sems.at[3, s], xpeer)

    def xf_in(s):
        slot = arrived.at[s, posx]
        return remote(slot, slot, sems.at[2, s], sems.at[3, s], xpeer)

    def cf(s):
        slab = arrived.at[s, pl.ds(mine, 2)]
        return remote(slab, slab, sems.at[4, s], sems.at[5, s], cpeer)

    def cf_in(s):
        slab = arrived.at[s, pl.ds(2 - mine, 2)]
        return remote(slab, slab, sems.at[4, s], sems.at[5, s], cpeer)

    def give_a(s):
        return remote(part.at[s, 1 - core], a_recv.at[s], sems.at[6, s], sems.at[7, s], cpeer)

    def give_b(s):
        return remote(b_send.at[s], b_recv.at[s], sems.at[8, s], sems.at[9, s], xpeer)

    def give_c(s):
        return remote(c_send.at[s], c_recv.at[ep], sems.at[10, s], sems.at[11, ep], {"ep": s})

    def give_c_in(e):
        return remote(c_recv.at[e], c_recv.at[e], sems.at[10, e], sems.at[11, e], {"ep": e})

    after = lax.rem(ep + 1, experts)
    prior = lax.rem(ep + experts - 1, experts)
    rim_out = remote(rim_send, rim_recv, t_sems.at[0, 0], t_sems.at[1, 0], {"ep": after})
    rim_in = remote(rim_recv, rim_recv, t_sems.at[0, 0], t_sems.at[1, 0], {"ep": prior})
    stat_out = [
        remote(stat_send, stat_recv.at[p], t_sems.at[0, p + 1], t_sems.at[1, p + 1], peer)
        for p, peer in enumerate((xpeer, cpeer, dpeer))
    ]
    mix_a = remote(m_part.at[1 - core], m_a, m_sems.at[0, 0], m_sems.at[1, 0], cpeer)
    half = rows // 2
    mix_b = [
        remote(
            m_bs.at[pl.ds(h * half, half)], m_b.at[pl.ds(h * half, half)],
            m_sems.at[2, h], m_sems.at[3, h], xpeer,
        )
        for h in range(2)
    ]

    pl.semaphore_wait(barrier, experts + 2)
    rim_out.start()

    @pl.loop(1, groups)
    def _(q):
        send_table(q).start()

    for b in range(2):
        pick = selected([slots[b, grp * NEAR + m] for m in range(NEAR)])
        where = side if b == 0 else 1 - side
        for n in range(0, width, tile):
            y = jnp.dot(pick, normed[b, :, n : n + tile], preferred_element_type=F32)
            near_pack[:, where, :, n : n + tile] = y.reshape(NEAR, cap, tile).astype(BF16)

    arrived[ep, pl.ds(mine, 2)] = near_pack[mem]
    send_near(1).start()
    cf(ep).start()

    @pl.loop(1, groups)
    def _(q):
        send_tokens(q).start()

    send_near(2).start()

    strips = chans // LANES

    @pl.loop(0, length // 64)
    def _(r):
        here = pl.multiple_of(r * 64, 64)
        for lane in range(strips):
            at = slice(lane * LANES, (lane + 1) * LANES)
            padded[lane, pl.ds(here + RIM, 64)] = gated(here, 64, at).astype(F32)

    def ffn(s):
        x = joined(arrived[s])
        gate = jnp.minimum(jnp.dot(x, gate_w[...], preferred_element_type=F32), LIMIT)
        lin = jnp.clip(jnp.dot(x, lin_w[...], preferred_element_type=F32), -LIMIT, LIMIT)
        hidden = (gate * jax.nn.sigmoid(SLOPE * gate) * (lin + 1.0)).astype(BF16)
        for n in range(0, width, tile):
            y = jnp.dot(hidden, down_w[:, n : n + tile], preferred_element_type=F32)
            part[s, :, :, :, n : n + tile] = y.reshape(2, 2, cap, tile).astype(BF16)

    def convolve():
        rim_in.wait_recv()
        open_rim = jnp.where(ep > 0, 1.0, 0.0)
        for lane in range(strips):
            padded[lane, 0:RIM] = (
                rim_recv[:, lane * LANES : (lane + 1) * LANES].astype(F32) * open_rim
            )

        @pl.loop(0, length // 64)
        def _(r):
            here = pl.multiple_of(r * 64, 64)
            sums = jnp.zeros((64, LANES), F32)
            squares = jnp.zeros((64, LANES), F32)
            for lane in range(strips):
                value_sum = jnp.zeros((64, LANES), F32)
                for tap in range(taps):
                    value_sum = value_sum + (
                        kern[tap : tap + 1, lane * LANES : (lane + 1) * LANES]
                        * padded[lane, pl.ds(here + (RIM - taps + 1 + tap), 64)]
                    )
                conv[lane, pl.ds(here, 64)] = value_sum
                sums = sums + value_sum
                squares = squares + value_sum * value_sum
            tot[pl.ds(here, 64)] = sums
            squ[pl.ds(here, 64)] = squares

        blocks = length // rows
        for t in range(blocks):
            at = slice(t * rows, (t + 1) * rows)
            stat_send[t : t + 1] = jnp.sum(tot[at].T, axis=0, keepdims=True)
            stat_send[blocks + t : blocks + t + 1] = jnp.sum(squ[at].T, axis=0, keepdims=True)
        for copy in stat_out:
            copy.start()

    def mix():
        for copy in stat_out:
            copy.wait_recv()
        stats = stat_send[...] + stat_recv[0] + stat_recv[1] + stat_recv[2]
        blocks = length // rows
        mean = stats[:blocks] / (chans * 4)
        var = stats[blocks:] / (chans * 4) - mean * mean
        scale = lax.rsqrt(var + EPS)
        for t in range(blocks):
            at = slice(t * rows, (t + 1) * rows)
            middle = jnp.broadcast_to(mean[t : t + 1], (LANES, rows)).T
            spread = jnp.broadcast_to(scale[t : t + 1], (LANES, rows)).T
            for lane in range(strips):
                over = slice(lane * LANES, (lane + 1) * LANES)
                centred = (conv[lane, at] - middle) * spread * ngain[:, over]
                act[at, over] = jax.nn.silu(centred).astype(BF16)
        loads[7].wait()
        for n in range(0, width, tile):
            y = jnp.dot(act[...], proj_w[:, n : n + tile], preferred_element_type=F32)
            for t in range(4):
                m_part[t % 2, t // 2, :, n : n + tile] = y[t * rows : (t + 1) * rows].astype(BF16)
        mix_a.start()

    def due(i, late, step):
        at = i - late

        @pl.when(jnp.logical_and(at >= 0, at < experts))
        def _():
            step(source(at))

    def expert_step(s):
        cf_in(s).wait_recv()
        ffn(s)
        give_a(s).start()

    def first_sum(s):
        give_a(s).wait_recv()
        b_send[s] = (part[s, core, 1 - side].astype(F32) + a_recv[s, 1 - side].astype(F32)).astype(BF16)
        give_b(s).start()

    def second_sum(s):
        give_b(s).wait_recv()
        total = part[s, core, side].astype(F32) + a_recv[s, side].astype(F32) + b_recv[s].astype(F32)

        @pl.when(s == ep)
        def _():
            c_recv[s] = total.astype(BF16)

        @pl.when(s != ep)
        def _():
            c_send[s] = total.astype(BF16)
            give_c(s).start()

    for load in loads[4:7]:
        load.wait()

    def lay_weights():
        order = lax.broadcasted_iota(jnp.int32, (cap, rows), 0).astype(F32)
        for group in range(groups):
            stacked = jnp.concatenate(
                [
                    jnp.where(slots[0, e] == order, weights[e], 0.0)
                    for e in range(group * NEAR, group * NEAR + NEAR)
                ],
                axis=0,
            ).T
            high = stacked.astype(BF16)
            wmat[0, group] = high
            wmat[1, group] = (stacked - high.astype(F32)).astype(BF16)

    def arrival(i, s):
        @pl.when(near_step(i))
        def _():
            near_in(s).wait_recv()
            cf(s).start()

        @pl.when(jnp.logical_not(near_step(i)))
        def _():
            xf_in(s).wait_recv()
            cf(s).start()

    @pl.loop(1, experts + 2)
    def _(i):
        @pl.when(i == 2)
        def _():
            mix_a.wait_recv()
            m_bs[...] = (m_part[core, 1 - side].astype(F32) + m_a[1 - side].astype(F32)).astype(BF16)
            mix_b[0].start()

        due(i, 1, expert_step)

        @pl.when(i == 1)
        def _():
            convolve()

        due(i, 1, first_sum)

        @pl.when(i == 1)
        def _():
            mix()

        @pl.when(i == 2)
        def _():
            lay_weights()

            @pl.loop(1, groups)
            def _(q):
                relay(lax.rem(grp + q, groups))

        @pl.when(jnp.logical_and(i > 1, i < experts - 2))
        def _():
            j = i - 2
            s = far_source(j)

            @pl.when(lax.rem(j, NEAR) > 0)
            def _():
                far_in(s).wait_recv()

            xf(s).start()

        @pl.when(i == 4)
        def _():
            send_near(3).start()

        @pl.when(i == experts)
        def _():
            mix_b[1].start()

        due(i, 2, second_sum)
        due(i, 0, lambda s: arrival(i, s))

    for copy in mix_b:
        copy.wait_recv()
    mix_out[...] = (
        m_part[core, side].astype(F32) + m_a[side].astype(F32) + m_b[...].astype(F32)
    )

    def weighted(group, n):
        results = joined(c_recv[pl.ds(group * NEAR, NEAR), :, n : n + tile])
        return jnp.dot(wmat[0, group], results, preferred_element_type=F32) + jnp.dot(
            wmat[1, group], results, preferred_element_type=F32
        )

    for k in range(1, NEAR):
        give_c_in(near(k)).wait_recv()
    for n in range(0, width, tile):
        summed[:, n : n + tile] = weighted(grp, n)

    @pl.loop(1, groups - 1)
    def _(q):
        other = lax.rem(grp + q, groups)
        for m in range(NEAR):
            give_c_in(other * NEAR + m).wait_recv()
        for n in range(0, width, tile):
            summed[:, n : n + tile] += weighted(other, n)

    last = lax.rem(grp + groups - 1, groups)
    for m in range(NEAR):
        give_c_in(last * NEAR + m).wait_recv()
    for n in range(0, width, tile):
        moe_out[:, n : n + tile] = summed[:, n : n + tile] + weighted(last, n)

    mix_a.wait_send()
    for copy in mix_b:
        copy.wait_send()
    rim_out.wait_send()
    for copy in stat_out:
        copy.wait_send()
    for k in range(1, NEAR):
        send_near(k).wait_send()

    @pl.loop(1, groups)
    def _(q):
        send_table(q).wait_send()
        send_tokens(q).wait_send()
        for k in range(1, NEAR):
            send_relayed(lax.rem(grp + q, groups), k).wait_send()

    @pl.loop(0, experts - NEAR)
    def _(j):
        xf(far_source(j)).wait_send()

    @pl.loop(0, experts)
    def _(s):
        @pl.when(s != ep)
        def _():
            give_c(s).wait_send()

        cf(s).wait_send()
        give_a(s).wait_send()
        give_b(s).wait_send()


def shards(
    conv_value,
    conv_gate,
    conv_kernel,
    norm_gain,
    mixer_proj,
    moe_in,
    route_ids,
    route_logits,
    moe_gain,
    expert_gate,
    expert_lin,
    expert_down,
):
    tp_size = lax.axis_size("tp")
    experts = lax.axis_size("ep")
    tokens, width = moe_in.shape
    rows = tokens // tp_size
    topk = route_ids.shape[1]
    capacity = max(2, 2 * rows * topk // experts)
    hid = expert_gate.shape[2]
    length, chans = conv_value.shape
    padded_experts = -(-experts // 8) * 8
    if tp_size != 4 or experts % NEAR or topk != 2 or length != tokens or rows != LANES:
        raise ValueError("unsupported sizes")

    def by_block(table):
        return table.reshape(tp_size, rows, topk).transpose(0, 2, 1)

    vmem = pl.BlockSpec(memory_space=pltpu.VMEM)
    hbm = pl.BlockSpec(memory_space=pl.ANY)
    out = jax.ShapeDtypeStruct((rows, width), F32)
    slot_rows = (experts, capacity, width)
    mixer_out, moe_out = pl.pallas_call(
        layer_kernel,
        out_shape=(out, out),
        in_specs=[vmem] * 5 + [hbm] * 7,
        out_specs=(vmem, vmem),
        scratch_shapes=[
            pltpu.VMEM((width, hid), BF16),
            pltpu.VMEM((width, hid), BF16),
            pltpu.VMEM((hid, width), BF16),
            pltpu.VMEM((chans, width), BF16),
            pltpu.VMEM((2, rows, width), BF16),
            pltpu.VMEM((2, rows, width), BF16),
            pltpu.VMEM((2, padded_experts, 1, rows), F32),
            pltpu.VMEM((padded_experts, 1, rows), F32),
            pltpu.VMEM(slot_rows, BF16),
            pltpu.VMEM((NEAR, 2, capacity, width), BF16),
            pltpu.VMEM((experts // NEAR, rows, width), BF16),
            pltpu.VMEM((experts // NEAR, NEAR, 1, rows), F32),
            pltpu.VMEM((experts, tp_size, capacity, width), BF16),
            pltpu.VMEM((experts, 2, 2, capacity, width), BF16),
            pltpu.VMEM((experts, 2, capacity, width), BF16),
            pltpu.VMEM(slot_rows, BF16),
            pltpu.VMEM(slot_rows, BF16),
            pltpu.VMEM(slot_rows, BF16),
            pltpu.VMEM(slot_rows, BF16),
            pltpu.VMEM((length, chans), BF16),
            pltpu.VMEM((length, chans), BF16),
            pltpu.VMEM((chans // LANES, length + RIM, LANES), F32),
            pltpu.VMEM((chans // LANES, length, LANES), F32),
            pltpu.VMEM((length, LANES), F32),
            pltpu.VMEM((length, LANES), F32),
            pltpu.VMEM((length, chans), BF16),
            pltpu.VMEM((RIM, chans), BF16),
            pltpu.VMEM((RIM, chans), BF16),
            pltpu.VMEM((8, LANES), F32),
            pltpu.VMEM((3, 8, LANES), F32),
            pltpu.VMEM((2, 2, rows, width), BF16),
            pltpu.VMEM((2, rows, width), BF16),
            pltpu.VMEM((rows, width), BF16),
            pltpu.VMEM((rows, width), BF16),
            pltpu.VMEM((2, experts // NEAR, rows, NEAR * capacity), BF16),
            pltpu.VMEM((rows, width), F32),
            pltpu.SemaphoreType.DMA((8,)),
            pltpu.SemaphoreType.DMA((12, experts)),
            pltpu.SemaphoreType.DMA((2, 4)),
            pltpu.SemaphoreType.DMA((4, 2)),
            pltpu.SemaphoreType.DMA((4, experts // NEAR)),
        ],
        compiler_params=pltpu.CompilerParams(
            has_side_effects=True, collective_id=0, vmem_limit_bytes=62 * 1024 * 1024
        ),
    )(
        by_block(route_ids), by_block(route_logits), conv_kernel, norm_gain[None], moe_gain[None],
        moe_in, conv_value, conv_gate, expert_gate[0], expert_lin[0], expert_down[0], mixer_proj,
    )
    return (mixer_out.astype(BF16), moe_out.astype(BF16))


def solution(mesh):
    placed = (
        P("ep", "tp"),
        P("ep", "tp"),
        P(None, "tp"),
        P("tp"),
        P("tp", None),
        P("ep", None),
        P("ep", None),
        P("ep", None),
        P(),
        P("ep", None, "tp"),
        P("ep", None, "tp"),
        P("ep", "tp", None),
    )
    return jax.shard_map(
        shards,
        mesh=mesh,
        in_specs=placed,
        out_specs=(P(("ep", "tp"), None), P(("ep", "tp"), None)),
        check_vma=False,
    )
```

```python
import jax
import jax.numpy as jnp
from jax import lax
from jax.experimental import pallas as pl
from jax.experimental.pallas import tpu as pltpu
from jax.sharding import PartitionSpec as P

EPS = 1e-05
LIMIT = 7.0
SLOPE = 1.702
F32 = jnp.float32
BF16 = jnp.bfloat16
LANES = 128
RIM = 32
NEAR = 4


def remote(src, dst, send, recv, device):
    return pltpu.make_async_remote_copy(
        src_ref=src,
        dst_ref=dst,
        send_sem=send,
        recv_sem=recv,
        device_id=device,
        device_id_type=pl.DeviceIdType.MESH,
    )


def joined(block):
    groups, rows, width = block.shape
    if rows % 16:
        return block.astype(F32).reshape(groups * rows, width).astype(BF16)
    return block.reshape(groups * rows, width)


def layer_kernel(
    ids, logits, kern, ngain, mgain,
    moe_hbm, value_hbm, cgate_hbm, gate_hbm, lin_hbm, down_hbm, proj_hbm,
    mix_out, moe_out,
    gate_w, lin_w, down_w, proj_w,
    xrows, normed, slots, weights, far_pack, near_pack, tokens, table,
    arrived, part, a_recv, b_send, b_recv, c_send, c_recv,
    value, cgate, padded, conv, tot, squ, act, rim_send, rim_recv, stat_send, stat_recv,
    m_part, m_a, m_bs, m_b,
    wmat, summed, mix_stage, load_sem, sems, t_sems, m_sems, g_sems,
):
    experts, _, cap, width = arrived.shape
    rows = moe_out.shape[0]
    length, chans = value.shape
    taps = kern.shape[0]
    groups = experts // NEAR
    ep, tp = lax.axis_index("ep"), lax.axis_index("tp")
    core, side = lax.rem(tp, 2), lax.div(tp, 2)
    xpeer, cpeer = {"tp": lax.rem(tp + 2, 4)}, {"tp": tp + 1 - 2 * core}
    dpeer = {"tp": lax.rem(tp + 3 - 2 * core, 4)}
    pos, posx = core * 2 + side, core * 2 + 1 - side
    mine = core * 2
    grp = lax.div(ep, NEAR)
    mem = lax.rem(ep, NEAR)
    row, col = lax.div(mem, 2), lax.rem(mem, 2)
    mirror = (1 - row) * 2 + col
    outer = row == lax.rem(grp, 2)

    def near(k):
        return grp * NEAR + lax.rem(row + k // 2, 2) * 2 + lax.rem(col + k, 2)

    def far_source(j):
        other = lax.rem(grp + lax.div(j, NEAR) + 1, groups)
        k = lax.rem(j, NEAR)
        return other * NEAR + lax.rem(row + 1 + lax.div(k, 2), 2) * 2 + lax.rem(col + k, 2)

    def near_step(i):
        return jnp.logical_or(i < 3, i == experts - 2)

    def source(i):
        k = jnp.minimum(i, 3)
        close = grp * NEAR + lax.rem(row + lax.div(k, 2), 2) * 2 + lax.rem(col + k, 2)
        distant = far_source(jnp.where(i == experts - 1, i - NEAR, jnp.maximum(i - 3, 0)))
        return jnp.where(near_step(i), close, distant)

    loads = [
        pltpu.make_async_copy(moe_hbm.at[pl.ds(tp * rows, rows)], xrows.at[0], load_sem.at[0]),
        pltpu.make_async_copy(
            moe_hbm.at[pl.ds(lax.rem(tp + 2, 4) * rows, rows)], xrows.at[1], load_sem.at[1]
        ),
        pltpu.make_async_copy(value_hbm, value, load_sem.at[2]),
        pltpu.make_async_copy(cgate_hbm, cgate, load_sem.at[3]),
        pltpu.make_async_copy(gate_hbm, gate_w, load_sem.at[4]),
        pltpu.make_async_copy(lin_hbm, lin_w, load_sem.at[5]),
        pltpu.make_async_copy(down_hbm, down_w, load_sem.at[6]),
        pltpu.make_async_copy(proj_hbm, proj_w, load_sem.at[7]),
    ]
    for load in loads:
        load.start()

    barrier = pltpu.get_barrier_semaphore()

    @pl.loop(1, experts)
    def _(d):
        pl.semaphore_signal(
            barrier, inc=1, device_id={"ep": lax.rem(ep + d, experts)},
            device_id_type=pl.DeviceIdType.MESH,
        )

    for peer in (xpeer, cpeer, dpeer):
        pl.semaphore_signal(barrier, inc=1, device_id=peer, device_id_type=pl.DeviceIdType.MESH)

    padded_experts = -(-experts // 8) * 8
    before = (
        lax.broadcasted_iota(jnp.int32, (rows, rows), 0)
        < lax.broadcasted_iota(jnp.int32, (rows, rows), 1)
    ).astype(BF16)
    names = lax.broadcasted_iota(jnp.int32, (padded_experts, rows), 0)
    for b, block in ((0, tp), (1, lax.rem(tp + 2, 4))):
        chosen = ids[block]
        first, second = chosen[0:1] == names, chosen[1:2] == names
        taken = jnp.where(jnp.logical_or(first, second), 1.0, 0.0)
        rank = jnp.dot(taken.astype(BF16), before, preferred_element_type=F32)
        place = jnp.where(taken > 0.0, rank, -1.0)
        for e in range(experts):
            slots[b, e] = place[e : e + 1]
        if b == 0:
            expo = jnp.exp(logits[block])
            total = expo[0:1] + expo[1:2]
            share = jnp.where(first, expo[0:1] / total, 0.0) + jnp.where(
                second, expo[1:2] / total, 0.0
            )
            for e in range(experts):
                weights[e] = share[e : e + 1]

    def selected(places):
        order = lax.broadcasted_iota(jnp.int32, (cap, rows), 0).astype(F32)
        picks = [jnp.where(place == order, 1.0, 0.0) for place in places]
        return jnp.concatenate(picks, axis=0).astype(BF16)

    for b in range(2):
        loads[b].wait()
        for r in range(0, rows, 16):
            block = xrows[b, r : r + 16].astype(F32)
            mu = jnp.mean(block, axis=1, keepdims=True)
            block = block - mu
            va = jnp.mean(jnp.square(block), axis=1, keepdims=True)
            normed[b, r : r + 16] = (block * lax.rsqrt(va + EPS) * mgain[...]).astype(BF16)

    tile = min(512, width)
    def gated(start, count, over):
        glu = value[pl.ds(start, count), over].astype(F32) * jax.nn.sigmoid(
            cgate[pl.ds(start, count), over].astype(F32)
        )
        return glu.astype(BF16)

    loads[2].wait()
    loads[3].wait()
    rim_send[...] = gated(length - RIM, RIM, slice(None))

    def send_near(k):
        e = near(k)
        return remote(
            near_pack.at[lax.rem(e, NEAR)], arrived.at[ep, pl.ds(mine, 2)],
            sems.at[0, e], sems.at[1, ep], {"ep": e},
        )

    def near_in(s):
        slab = arrived.at[s, pl.ds(mine, 2)]
        return remote(slab, slab, sems.at[0, s], sems.at[1, s], {"ep": s})

    def send_tokens(q):
        other = lax.rem(grp + q, groups)
        return remote(
            normed.at[0], tokens.at[grp], g_sems.at[0, other], g_sems.at[1, grp],
            {"ep": other * NEAR + mirror},
        )

    def tokens_in(other):
        return remote(
            tokens.at[other], tokens.at[other], g_sems.at[0, other], g_sems.at[1, other], {"ep": other * NEAR + mirror}
        )

    def send_table(q):
        other = lax.rem(grp + q, groups)
        return remote(
            slots.at[0, pl.ds(other * NEAR, NEAR)], table.at[grp],
            g_sems.at[2, other], g_sems.at[3, grp], {"ep": other * NEAR + mirror},
        )

    def table_in(other):
        return remote(
            table.at[other], table.at[other], g_sems.at[2, other], g_sems.at[3, other], {"ep": other * NEAR + mirror}
        )

    def send_relayed(other, k):
        e = near(k)
        place = other * NEAR + lax.rem(e, NEAR)
        return remote(
            far_pack.at[place], arrived.at[other * NEAR + mirror, pos],
            sems.at[0, place], sems.at[1, other * NEAR + mirror], {"ep": e},
        )

    def relay(other):
        tokens_in(other).wait_recv()
        table_in(other).wait_recv()
        pick = selected([table[other, m] for m in range(NEAR)])
        for n in range(0, width, tile):
            y = jnp.dot(pick, tokens[other, :, n : n + tile], preferred_element_type=F32)
            far_pack[pl.ds(other * NEAR, NEAR), :, n : n + tile] = y.reshape(
                NEAR, cap, tile
            ).astype(BF16)
        for k in range(1, NEAR - 1):
            send_relayed(other, k).start()
        arrived[other * NEAR + mirror, pos] = far_pack[other * NEAR + mem]

    def far_in(s):
        slot = arrived.at[s, pos]
        return remote(slot, slot, sems.at[0, s], sems.at[1, s], {"ep": s})

    def xf(s):
        slot = arrived.at[s, pos]
        return remote(slot, slot, sems.at[2, s], sems.at[3, s], xpeer)

    def xf_in(s):
        slot = arrived.at[s, posx]
        return remote(slot, slot, sems.at[2, s], sems.at[3, s], xpeer)

    def cf(s):
        slab = arrived.at[s, pl.ds(mine, 2)]
        return remote(slab, slab, sems.at[4, s], sems.at[5, s], cpeer)

    def cf_in(s):
        slab = arrived.at[s, pl.ds(2 - mine, 2)]
        return remote(slab, slab, sems.at[4, s], sems.at[5, s], cpeer)

    def give_a(s):
        return remote(part.at[s, 1 - core], a_recv.at[s], sems.at[6, s], sems.at[7, s], cpeer)

    def give_b(s):
        return remote(b_send.at[s], b_recv.at[s], sems.at[8, s], sems.at[9, s], xpeer)

    def give_c(s):
        return remote(c_send.at[s], c_recv.at[ep], sems.at[10, s], sems.at[11, ep], {"ep": s})

    def give_c_in(e):
        return remote(c_recv.at[e], c_recv.at[e], sems.at[10, e], sems.at[11, e], {"ep": e})

    after = lax.rem(ep + 1, experts)
    prior = lax.rem(ep + experts - 1, experts)
    rim_out = remote(rim_send, rim_recv, t_sems.at[0, 0], t_sems.at[1, 0], {"ep": after})
    rim_in = remote(rim_recv, rim_recv, t_sems.at[0, 0], t_sems.at[1, 0], {"ep": prior})
    stat_out = [
        remote(stat_send, stat_recv.at[p], t_sems.at[0, p + 1], t_sems.at[1, p + 1], peer)
        for p, peer in enumerate((xpeer, cpeer, dpeer))
    ]
    mix_a = remote(m_part.at[1 - core], m_a, m_sems.at[0, 0], m_sems.at[1, 0], cpeer)
    half = rows // 2
    mix_b = [
        remote(
            m_bs.at[pl.ds(h * half, half)], m_b.at[pl.ds(h * half, half)],
            m_sems.at[2, h], m_sems.at[3, h], xpeer,
        )
        for h in range(2)
    ]

    pl.semaphore_wait(barrier, experts + 2)
    rim_out.start()

    @pl.loop(1, groups)
    def _(q):
        send_table(q).start()

    for b in range(2):
        pick = selected([slots[b, grp * NEAR + m] for m in range(NEAR)])
        where = side if b == 0 else 1 - side
        for n in range(0, width, tile):
            y = jnp.dot(pick, normed[b, :, n : n + tile], preferred_element_type=F32)
            near_pack[:, where, :, n : n + tile] = y.reshape(NEAR, cap, tile).astype(BF16)

    arrived[ep, pl.ds(mine, 2)] = near_pack[mem]
    send_near(1).start()
    cf(ep).start()

    @pl.loop(1, groups)
    def _(q):
        send_tokens(q).start()

    send_near(2).start()

    strips = chans // LANES

    @pl.loop(0, length // 64)
    def _(r):
        here = pl.multiple_of(r * 64, 64)
        for lane in range(strips):
            at = slice(lane * LANES, (lane + 1) * LANES)
            padded[lane, pl.ds(here + RIM, 64)] = gated(here, 64, at).astype(F32)

    def ffn(s):
        x = joined(arrived[s])
        gate = jnp.minimum(jnp.dot(x, gate_w[...], preferred_element_type=F32), LIMIT)
        lin = jnp.clip(jnp.dot(x, lin_w[...], preferred_element_type=F32), -LIMIT, LIMIT)
        hidden = (gate * jax.nn.sigmoid(SLOPE * gate) * (lin + 1.0)).astype(BF16)
        for n in range(0, width, tile):
            y = jnp.dot(hidden, down_w[:, n : n + tile], preferred_element_type=F32)
            part[s, :, :, :, n : n + tile] = y.reshape(2, 2, cap, tile).astype(BF16)

    def conv_rows(r):
        here = pl.multiple_of(r * 64, 64) if not isinstance(r, int) else r * 64
        sums = jnp.zeros((64, LANES), F32)
        squares = jnp.zeros((64, LANES), F32)
        for lane in range(strips):
            value_sum = jnp.zeros((64, LANES), F32)
            for tap in range(taps):
                value_sum = value_sum + (
                    kern[tap : tap + 1, lane * LANES : (lane + 1) * LANES]
                    * padded[lane, pl.ds(here + (RIM - taps + 1 + tap), 64)]
                )
            conv[lane, pl.ds(here, 64)] = value_sum
            sums = sums + value_sum
            squares = squares + value_sum * value_sum
        tot[pl.ds(here, 64)] = sums
        squ[pl.ds(here, 64)] = squares

    @pl.loop(1, length // 64)
    def _(r):
        conv_rows(r)

    def convolve():
        rim_in.wait_recv()
        open_rim = jnp.where(ep > 0, 1.0, 0.0)
        for lane in range(strips):
            padded[lane, 0:RIM] = (
                rim_recv[:, lane * LANES : (lane + 1) * LANES].astype(F32) * open_rim
            )

        conv_rows(0)
        blocks = length // rows
        for t in range(blocks):
            at = slice(t * rows, (t + 1) * rows)
            stat_send[t : t + 1] = jnp.sum(tot[at].T, axis=0, keepdims=True)
            stat_send[blocks + t : blocks + t + 1] = jnp.sum(squ[at].T, axis=0, keepdims=True)
        for copy in stat_out:
            copy.start()

    def mix():
        for copy in stat_out:
            copy.wait_recv()
        stats = stat_send[...] + stat_recv[0] + stat_recv[1] + stat_recv[2]
        blocks = length // rows
        mean = stats[:blocks] / (chans * 4)
        var = stats[blocks:] / (chans * 4) - mean * mean
        scale = lax.rsqrt(var + EPS)
        for t in range(blocks):
            at = slice(t * rows, (t + 1) * rows)
            middle = jnp.broadcast_to(mean[t : t + 1], (LANES, rows)).T
            spread = jnp.broadcast_to(scale[t : t + 1], (LANES, rows)).T
            for lane in range(strips):
                over = slice(lane * LANES, (lane + 1) * LANES)
                centred = (conv[lane, at] - middle) * spread * ngain[:, over]
                act[at, over] = jax.nn.silu(centred).astype(BF16)
        loads[7].wait()
        for n in range(0, width, tile):
            y = jnp.dot(act[...], proj_w[:, n : n + tile], preferred_element_type=F32)
            for t in range(4):
                m_part[t % 2, t // 2, :, n : n + tile] = y[t * rows : (t + 1) * rows].astype(BF16)
        mix_a.start()

    def due(i, late, step):
        at = i - late

        @pl.when(jnp.logical_and(at >= 0, at < experts))
        def _():
            step(source(at))

    def expert_step(s):
        cf_in(s).wait_recv()
        ffn(s)
        give_a(s).start()

    def first_sum(s):
        give_a(s).wait_recv()
        b_send[s] = (part[s, core, 1 - side].astype(F32) + a_recv[s, 1 - side].astype(F32)).astype(BF16)
        give_b(s).start()

    def second_sum(s):
        give_b(s).wait_recv()
        total = part[s, core, side].astype(F32) + a_recv[s, side].astype(F32) + b_recv[s].astype(F32)

        @pl.when(s == ep)
        def _():
            c_recv[s] = total.astype(BF16)

        @pl.when(s != ep)
        def _():
            c_send[s] = total.astype(BF16)
            give_c(s).start()

    for load in loads[4:7]:
        load.wait()

    def lay_weights():
        order = lax.broadcasted_iota(jnp.int32, (cap, rows), 0).astype(F32)
        for group in range(groups):
            stacked = jnp.concatenate(
                [
                    jnp.where(slots[0, e] == order, weights[e], 0.0)
                    for e in range(group * NEAR, group * NEAR + NEAR)
                ],
                axis=0,
            ).T
            high = stacked.astype(BF16)
            wmat[0, group] = high
            wmat[1, group] = (stacked - high.astype(F32)).astype(BF16)

    def arrival(i, s):
        @pl.when(near_step(i))
        def _():
            near_in(s).wait_recv()
            cf(s).start()

        @pl.when(jnp.logical_not(near_step(i)))
        def _():
            xf_in(s).wait_recv()
            cf(s).start()

    @pl.loop(1, experts + 2)
    def _(i):
        @pl.when(i == 2)
        def _():
            mix_a.wait_recv()
            m_bs[...] = (m_part[core, 1 - side].astype(F32) + m_a[1 - side].astype(F32)).astype(BF16)
            mix_b[0].start()

        due(i, 1, expert_step)

        @pl.when(i == 1)
        def _():
            convolve()

        due(i, 1, first_sum)

        @pl.when(i == 1)
        def _():
            mix()

        @pl.when(i == 2)
        def _():
            lay_weights()

            @pl.loop(1, groups)
            def _(q):
                relay(lax.rem(grp + q, groups))

        @pl.when(jnp.logical_and(i > 1, i < experts - 2))
        def _():
            j = i - 2
            s = far_source(j)

            @pl.when(lax.rem(j, NEAR) > 0)
            def _():
                far_in(s).wait_recv()

            xf(s).start()

        @pl.when(i == jnp.where(outer, 3, 2))
        def _():
            @pl.loop(1, groups)
            def _(q):
                send_relayed(lax.rem(grp + q, groups), NEAR - 1).start()

        @pl.when(i == 4)
        def _():
            send_near(3).start()

        @pl.when(i == experts)
        def _():
            mix_b[1].start()

        due(i, 2, second_sum)
        due(i, 0, lambda s: arrival(i, s))

    for copy in mix_b:
        copy.wait_recv()
    mix_stage[...] = (
        m_part[core, side].astype(F32) + m_a[side].astype(F32) + m_b[...].astype(F32)
    )

    mix_store = pltpu.make_async_copy(mix_stage, mix_out, load_sem.at[0])
    mix_store.start()

    def weighted(group, n):
        results = joined(c_recv[pl.ds(group * NEAR, NEAR), :, n : n + tile])
        return jnp.dot(wmat[0, group], results, preferred_element_type=F32) + jnp.dot(
            wmat[1, group], results, preferred_element_type=F32
        )

    for k in range(1, NEAR):
        give_c_in(near(k)).wait_recv()
    for n in range(0, width, tile):
        summed[:, n : n + tile] = weighted(grp, n)

    @pl.loop(1, groups - 1)
    def _(q):
        other = lax.rem(grp + q, groups)
        for m in range(NEAR):
            give_c_in(other * NEAR + m).wait_recv()
        for n in range(0, width, tile):
            summed[:, n : n + tile] += weighted(other, n)

    last = lax.rem(grp + groups - 1, groups)
    for m in range(NEAR):
        give_c_in(last * NEAR + m).wait_recv()
    stores = []
    for n in range(0, width, tile):
        over = slice(n, n + tile)
        summed[:, over] += weighted(last, n)
        stores.append(
            pltpu.make_async_copy(
                summed.at[:, over], moe_out.at[:, over], load_sem.at[1 + n // tile]
            )
        )
        stores[-1].start()

    mix_store.wait()
    for store in stores:
        store.wait()
    mix_a.wait_send()
    for copy in mix_b:
        copy.wait_send()
    rim_out.wait_send()
    for copy in stat_out:
        copy.wait_send()
    for k in range(1, NEAR):
        send_near(k).wait_send()

    @pl.loop(1, groups)
    def _(q):
        send_table(q).wait_send()
        send_tokens(q).wait_send()
        for k in range(1, NEAR):
            send_relayed(lax.rem(grp + q, groups), k).wait_send()

    @pl.loop(0, experts - NEAR)
    def _(j):
        xf(far_source(j)).wait_send()

    @pl.loop(0, experts)
    def _(s):
        @pl.when(s != ep)
        def _():
            give_c(s).wait_send()

        cf(s).wait_send()
        give_a(s).wait_send()
        give_b(s).wait_send()


def shards(
    conv_value,
    conv_gate,
    conv_kernel,
    norm_gain,
    mixer_proj,
    moe_in,
    route_ids,
    route_logits,
    moe_gain,
    expert_gate,
    expert_lin,
    expert_down,
):
    tp_size = lax.axis_size("tp")
    experts = lax.axis_size("ep")
    tokens, width = moe_in.shape
    rows = tokens // tp_size
    topk = route_ids.shape[1]
    capacity = max(2, 2 * rows * topk // experts)
    hid = expert_gate.shape[2]
    length, chans = conv_value.shape
    padded_experts = -(-experts // 8) * 8
    if tp_size != 4 or experts % NEAR or topk != 2 or length != tokens or rows != LANES:
        raise ValueError("unsupported sizes")

    def by_block(table):
        return table.reshape(tp_size, rows, topk).transpose(0, 2, 1)

    vmem = pl.BlockSpec(memory_space=pltpu.VMEM)
    hbm = pl.BlockSpec(memory_space=pl.ANY)
    out = jax.ShapeDtypeStruct((rows, width), F32)
    slot_rows = (experts, capacity, width)
    mixer_out, moe_out = pl.pallas_call(
        layer_kernel,
        out_shape=(out, out),
        in_specs=[vmem] * 5 + [hbm] * 7,
        out_specs=(hbm, hbm),
        scratch_shapes=[
            pltpu.VMEM((width, hid), BF16),
            pltpu.VMEM((width, hid), BF16),
            pltpu.VMEM((hid, width), BF16),
            pltpu.VMEM((chans, width), BF16),
            pltpu.VMEM((2, rows, width), BF16),
            pltpu.VMEM((2, rows, width), BF16),
            pltpu.VMEM((2, padded_experts, 1, rows), F32),
            pltpu.VMEM((padded_experts, 1, rows), F32),
            pltpu.VMEM(slot_rows, BF16),
            pltpu.VMEM((NEAR, 2, capacity, width), BF16),
            pltpu.VMEM((experts // NEAR, rows, width), BF16),
            pltpu.VMEM((experts // NEAR, NEAR, 1, rows), F32),
            pltpu.VMEM((experts, tp_size, capacity, width), BF16),
            pltpu.VMEM((experts, 2, 2, capacity, width), BF16),
            pltpu.VMEM((experts, 2, capacity, width), BF16),
            pltpu.VMEM(slot_rows, BF16),
            pltpu.VMEM(slot_rows, BF16),
            pltpu.VMEM(slot_rows, BF16),
            pltpu.VMEM(slot_rows, BF16),
            pltpu.VMEM((length, chans), BF16),
            pltpu.VMEM((length, chans), BF16),
            pltpu.VMEM((chans // LANES, length + RIM, LANES), F32),
            pltpu.VMEM((chans // LANES, length, LANES), F32),
            pltpu.VMEM((length, LANES), F32),
            pltpu.VMEM((length, LANES), F32),
            pltpu.VMEM((length, chans), BF16),
            pltpu.VMEM((RIM, chans), BF16),
            pltpu.VMEM((RIM, chans), BF16),
            pltpu.VMEM((8, LANES), F32),
            pltpu.VMEM((3, 8, LANES), F32),
            pltpu.VMEM((2, 2, rows, width), BF16),
            pltpu.VMEM((2, rows, width), BF16),
            pltpu.VMEM((rows, width), BF16),
            pltpu.VMEM((rows, width), BF16),
            pltpu.VMEM((2, experts // NEAR, rows, NEAR * capacity), BF16),
            pltpu.VMEM((rows, width), F32),
            pltpu.VMEM((rows, width), F32),
            pltpu.SemaphoreType.DMA((8,)),
            pltpu.SemaphoreType.DMA((12, experts)),
            pltpu.SemaphoreType.DMA((2, 4)),
            pltpu.SemaphoreType.DMA((4, 2)),
            pltpu.SemaphoreType.DMA((4, experts // NEAR)),
        ],
        compiler_params=pltpu.CompilerParams(
            has_side_effects=True, collective_id=0, vmem_limit_bytes=62 * 1024 * 1024
        ),
    )(
        by_block(route_ids), by_block(route_logits), conv_kernel, norm_gain[None], moe_gain[None],
        moe_in, conv_value, conv_gate, expert_gate[0], expert_lin[0], expert_down[0], mixer_proj,
    )
    return (mixer_out.astype(BF16), moe_out.astype(BF16))


def solution(mesh):
    placed = (
        P("ep", "tp"),
        P("ep", "tp"),
        P(None, "tp"),
        P("tp"),
        P("tp", None),
        P("ep", None),
        P("ep", None),
        P("ep", None),
        P(),
        P("ep", None, "tp"),
        P("ep", None, "tp"),
        P("ep", "tp", None),
    )
    return jax.shard_map(
        shards,
        mesh=mesh,
        in_specs=placed,
        out_specs=(P(("ep", "tp"), None), P(("ep", "tp"), None)),
        check_vma=False,
    )
```
